32 devices in a mesh: ep: 8 (over z, x), tp: 4 (over y, core).
Axes of the slice: x: 2, y: 2, z: 4, core: 2. Of those that a mesh axis runs over, the one named last changes fastest.
Arguments:
- queries: bfloat16 [6144, 1024], P('ep', 'tp'), may hold values from -6.5 to 6.5
- keys: bfloat16 [6144, 1024], P('ep', 'tp'), may hold values from -6.5 to 6.5
- values: bfloat16 [6144, 1024], P('ep', 'tp'), may hold values from -6 to 6
- cum_gate: float32 [6144, 16], P('ep', 'tp'), may hold values from -770 to 0, as said below
- head_gain: float32 [1024], P('tp'), may hold values from 0.1 to 1.9
- moe_in: bfloat16 [1024, 2048], P('ep'), may hold values from -6 to 6
- ffn_gain: float32 [2048], replicated, may hold values from 0.1 to 1.9
- routes: int32 [1024, 4], P('ep'), may hold values from 0 to 31, all different within a row; in each aligned block of 128 rows (0 to 127, 128 to 255, ...) at most 24 rows name the same one
- route_weight: float32 [1024, 4], P('ep'), may hold values from 0.2 to 1.2
- expert_gate: bfloat16 [32, 1024, 2048], P('ep', 'tp'), may hold values from -0.125 to 0.125
- expert_up: bfloat16 [32, 1024, 2048], P('ep', 'tp'), may hold values from -0.125 to 0.125
- expert_down: bfloat16 [32, 1024, 2048], P('ep', 'tp'), may hold values from -0.25 to 0.25
- shared_gate: bfloat16 [512, 2048], P('tp'), may hold values from -0.125 to 0.125
- shared_up: bfloat16 [512, 2048], P('tp'), may hold values from -0.125 to 0.125
- shared_down: bfloat16 [512, 2048], P('tp'), may hold values from -0.375 to 0.375
Outputs:
- mixed: bfloat16 [6144, 1024], P('ep', 'tp')
- expert_out: bfloat16 [1024, 2048], P('ep', 'tp')
The draws below stay inside these ranges and needn't reach their ends.
Inputs may be any that keep to these rules, and one draw needn't show every extreme that they name: `routes`: in each aligned block of 128 rows (the tokens of one index of ep) no expert is named by more than 24 rows, a bound that some block reaches; a row names 4 different experts. Each head's cum_gate never rises from one position to the next.
All inputs are finite; a program needn't handle non-finite values.
Results may differ from the reference program's by a relative error of at most 0.019.
Values may be sent and summed in bfloat16 or wider, within the bound.
A program may use at most 128 MiB of HBM per device.

```python
import math
import jax
import jax.numpy as jnp
import numpy as np
from jax import lax

D = 2048
HEADS = 16
HEAD = 64
FF_E = 1024
SHARED = 512
TOP = 4
ROWS = 768
MROWS = 128
SEQ = 6144
QW = 1024
MTOK = 1024
EXPERTS = 32
CAP = 24
N_EP = 8
N_TP = 4


def plant_pairs(key):
    base = jax.random.fold_in(key, 7)
    streams = jax.random.split(base, 2)
    query_rows = jnp.clip(jax.random.normal(streams[0], (SEQ, QW), jnp.float32), -6.0, 6.0)
    key_rows = jnp.clip(jax.random.normal(streams[1], (SEQ, QW), jnp.float32), -6.0, 6.0)
    return (query_rows, key_rows)


def draw_queries(key, part):
    return plant_pairs(key)[0].astype(jnp.bfloat16)


def draw_keys(key, part):
    return plant_pairs(key)[1].astype(jnp.bfloat16)


def draw_cum_gate(key, part):
    base = jax.random.fold_in(key, 11)
    streams = jax.random.split(base, 6)
    order = jax.random.permutation(streams[0], HEADS)
    slow_heads = order >= HEADS // 2
    fast_rate = jnp.exp(jax.random.uniform(streams[1], (HEADS,), jnp.float32, math.log(1.0 / 100.0), math.log(1.0 / 30.0)))
    fading_speed = jnp.where(slow_heads, 0.6 / SEQ, fast_rate)
    extent_coefficient = jnp.exp(jax.random.uniform(streams[2], (SEQ // ROWS,), jnp.float32, math.log(0.5), math.log(2.0)))
    extent_coefficient = jnp.repeat(extent_coefficient, ROWS)
    approximate_guess = jax.random.uniform(streams[3], (SEQ, HEADS), jnp.float32, 0.3, 1.7)
    spots = jax.random.randint(streams[4], (3,), 0, SEQ)
    discarded_items = jax.random.uniform(streams[5], (3, HEADS), jnp.float32, 0.22, 0.5)
    agreement_tally = (jnp.arange(SEQ)[:, None] == spots[None, :]).astype(jnp.float32)
    spike_occurrences = jnp.dot(agreement_tally, discarded_items)
    objective_list = fading_speed[None, :] * approximate_guess * extent_coefficient[:, None] + spike_occurrences
    return -jnp.cumsum(objective_list, axis=0)


def spiked(drawn, stream_key, source, target, parts, factor):
    def block_of(position):
        return (jnp.arange(drawn.shape[position]) // (drawn.shape[position] // parts)).reshape((-1,) + (1,) * (drawn.ndim - 1 - position))

    first = jax.random.permutation(stream_key, parts)[block_of(target)]
    second = (block_of(target) + parts // 2) % parts
    return jnp.where((block_of(source) == first) | (block_of(source) == second), factor * drawn, drawn)


def levels(stream_key, extent, cuts, smallest, top_value):
    level, own = 1.0, jax.random.fold_in(stream_key, 6)
    for axis_at, shards_of in cuts:
        draws = jnp.exp(jax.random.uniform(jax.random.fold_in(own, axis_at), (shards_of,), jnp.float32, smallest / len(cuts), top_value / len(cuts)))
        level = level * jnp.repeat(draws, extent[axis_at] // shards_of).reshape([-1 if axis == axis_at else 1 for axis in range(len(extent))])
    return level


def assign_block(own_key, own, number, rows, number_of, top, bound, skew):
    sequence = jax.random.permutation(own_key, number_of)
    heavy_load, common = load_shares(number_of, rows * top, bound, skew, True), load_shares(number_of, rows * top, bound, skew, False)
    places = jnp.arange(number_of)

    def named(tallies, offset_by):
        used = int((tallies > 0).sum())
        fixed = max(1, used // 4)
        passed = fixed + (places - fixed + offset_by * (used - fixed)) % max(1, number_of - fixed)
        return jnp.zeros((number_of,), jnp.int32).at[sequence[jnp.where(places < fixed, places, passed)]].set(jnp.asarray(tallies, jnp.int32))

    tallies = jnp.where(number % 4 == 0, named(heavy_load, number // 4), named(common, number - number // 4 - 1))
    mixed = jax.random.permutation(jax.random.fold_in(own, 3), number_of)
    giver, sink = mixed[0:number_of // 2 * 2:2], mixed[1:number_of // 2 * 2:2]
    slack = jnp.minimum(tallies[giver] - 1, bound - tallies[sink]) // 2
    slack = jnp.where((giver == sequence[0]) | (sink == sequence[0]) | (tallies[sink] == 0), 0, jnp.maximum(slack, 0))
    passed = jax.random.randint(jax.random.fold_in(own, 4), (number_of // 2,), 0, 1 << 20) % (slack + 1)
    tallies = tallies.at[giver].add(-passed).at[sink].add(passed)
    labels = jnp.searchsorted(jnp.cumsum(tallies), jnp.arange(rows * top), side="right").astype(jnp.int32)
    listing = labels.reshape(top, rows).T
    listing = listing[jax.random.permutation(jax.random.fold_in(own, 1), rows)]
    offset_by = jax.random.randint(jax.random.fold_in(own, 2), (rows, 1), 0, top)
    return jnp.take_along_axis(listing, (jnp.arange(top)[None, :] + offset_by) % top, axis=1)


def load_shares(amount, total, most, skew, full):
    portions = [(1 << 20) // math.isqrt(grade ** skew) + 1 for grade in range(1, amount + 1)]
    largest = most if full else min(most, max(-(-total // amount), total * portions[0] // sum(portions)))
    least = 1 if total - largest >= amount - 1 else 0
    counts, spare = [largest] + [least] * (amount - 1), total - largest - least * (amount - 1)
    while spare > 0:
        movable = [i for i in range(1, amount) if counts[i] < largest] or [i for i in range(1, amount) if counts[i] < most]
        whole, left = sum([portions[i] for i in movable]), spare
        for i in movable:
            more = min(most - counts[i], max(1, left * portions[i] // whole), spare)
            counts[i] = counts[i] + more
            spare = spare - more
    return np.array(counts)


def centred(own_key, extent, deviation, bound, cuts=(), kind=jnp.bfloat16):
    factor_of = levels(own_key, extent, cuts, -0.22, 0.18) if cuts else 1.0
    entries = jax.random.normal(own_key, extent, jnp.float32) * deviation * factor_of
    return jnp.minimum(jnp.maximum(entries, -bound), bound).astype(kind)


def gaussian_with(key, dims, width, bound, shards, heavy, kind=jnp.bfloat16):
    entries = width * jax.random.normal(key, dims, jnp.float32)
    if shards:
        entries = entries * levels(key, dims, shards, -0.22, 0.18)
    return jnp.clip(spiked(entries, jax.random.fold_in(key, 3), *heavy), -bound, bound).astype(kind)


def setup_inputs(seed: int = 0) -> dict:
    key_list = jax.random.split(jax.random.key(seed), 16)
    queries = draw_queries(jax.random.fold_in(key_list[15], 71), 0)
    keys = draw_keys(jax.random.fold_in(key_list[15], 71), 0)
    values = centred(key_list[2], (SEQ, QW), 1.0, 6.0, ((0, 8), (1, 4)))
    cum_gate = draw_cum_gate(jax.random.fold_in(key_list[15], 71), 0)
    head_gain = jnp.clip(1.0 + 0.18 * jax.random.normal(key_list[4], (QW,), jnp.float32), 0.1, 1.9)
    moe_in = centred(key_list[5], (MTOK, D), 1.0, 6.0, ((0, 8),))
    ffn_gain = jnp.clip(1.0 + 0.18 * jax.random.normal(key_list[6], (D,), jnp.float32), 0.1, 1.9)
    routes_keys = jax.random.split(jax.random.fold_in(key_list[7], 1), MTOK // MROWS)
    routes_turns = jax.random.permutation(jax.random.fold_in(key_list[7], 3), MTOK // MROWS)
    routes = jax.vmap(lambda own, number: assign_block(jax.random.fold_in(key_list[7], 2), own, number, MROWS, EXPERTS, TOP, CAP, 2))(routes_keys, routes_turns).reshape((MTOK, TOP))
    route_weight = jnp.clip(0.2 + 1 * jax.random.uniform(key_list[8], (MTOK, TOP), jnp.float32) ** levels(key_list[8], (MTOK, TOP), ((0, 8),), -0.2, 0.2), 0.2, 1.2)
    expert_gate = centred(key_list[9], (EXPERTS, FF_E, D), D ** -0.5, 0.125, ((0, 8), (1, 4)))
    expert_up = centred(key_list[10], (EXPERTS, FF_E, D), D ** -0.5, 0.125, ((0, 8), (1, 4)))
    expert_down = gaussian_with(key_list[11], (EXPERTS, FF_E, D), FF_E ** -0.5, 0.25, ((0, 8), (1, 4)), (1, 2, 4, 2.0))
    shared_gate = centred(key_list[12], (SHARED, D), D ** -0.5, 0.125, ((0, 4),))
    shared_up = centred(key_list[13], (SHARED, D), D ** -0.5, 0.125, ((0, 4),))
    shared_down = gaussian_with(key_list[14], (SHARED, D), SHARED ** -0.5, 0.375, ((0, 4),), (0, 1, 4, 2.0))
    return {"queries": queries, "keys": keys, "values": values, "cum_gate": cum_gate, "head_gain": head_gain, "moe_in": moe_in, "ffn_gain": ffn_gain, "routes": routes, "route_weight": route_weight, "expert_gate": expert_gate, "expert_up": expert_up, "expert_down": expert_down, "shared_gate": shared_gate, "shared_up": shared_up, "shared_down": shared_down}


NORM_EPSILON = 1e-06

def attend_head(head_inputs):
    query_head, key_head, value_head, gate_head = head_inputs
    block_len = math.gcd(SEQ, 512)
    positions = jnp.arange(SEQ, dtype=jnp.int32)
    score_scale = HEAD ** (-0.5)

    def one_block(block_num):
        first_row = block_num * block_len
        query_block = lax.dynamic_slice_in_dim(query_head, first_row, block_len, 0)
        gate_block = lax.dynamic_slice_in_dim(gate_head, first_row, block_len, 0)
        scores = jnp.dot(query_block, key_head.T, preferred_element_type=jnp.float32) * score_scale
        scores = scores + gate_block[:, None] - gate_head[None, :]
        query_pos = first_row + jnp.arange(block_len, dtype=jnp.int32)
        scores = jnp.where(positions[None, :] <= query_pos[:, None], scores, -jnp.inf)
        top_score = lax.optimization_barrier(jnp.max(scores, axis=1, keepdims=True))
        weights = jnp.exp(scores - top_score).astype(jnp.bfloat16)
        return jnp.dot(weights, value_head, preferred_element_type=jnp.float32)
    blocks = lax.map(one_block, jnp.arange(SEQ // block_len, dtype=jnp.int32))
    return blocks.reshape(SEQ, HEAD)

def blocked_down(hidden, weight):
    block_width = hidden.shape[1] // N_TP

    def add_block(running, block_num):
        start_col = block_num * block_width
        product = jnp.dot(lax.dynamic_slice_in_dim(hidden, start_col, block_width, 1), lax.dynamic_slice_in_dim(weight, start_col, block_width, 0), preferred_element_type=jnp.float32)
        rounded = lax.optimization_barrier(product.astype(jnp.bfloat16))
        return (running + rounded.astype(jnp.float32), None)
    start_sum = jnp.zeros((hidden.shape[0], weight.shape[1]), jnp.float32)
    result, _ = lax.scan(add_block, start_sum, jnp.arange(N_TP, dtype=jnp.int32))
    return result

def slot_index(route_rows):
    flat_routes = route_rows.reshape(-1)
    agreement_tally = (flat_routes[:, None] == jnp.arange(EXPERTS, dtype=jnp.int32)[None, :]).astype(jnp.int32)
    earlier = lax.optimization_barrier(jnp.sum((jnp.cumsum(agreement_tally, axis=0) - 1) * agreement_tally, axis=1))
    return (flat_routes * CAP + earlier).astype(jnp.int32)

def fill_slots(token_rows, slot_ids):
    owner_row = jnp.full((EXPERTS * CAP,), MROWS, jnp.int32).at[slot_ids].set(jnp.arange(MROWS * TOP, dtype=jnp.int32) // TOP)
    padded = jnp.concatenate([token_rows, jnp.zeros((1, D), token_rows.dtype)], axis=0)
    return padded[owner_row]

def run_expert(expert_inputs):
    rows_in, gate_weight, up_weight, down_weight = expert_inputs
    hidden = (jax.nn.silu(jnp.dot(rows_in, gate_weight.T, preferred_element_type=jnp.float32)) * jnp.dot(rows_in, up_weight.T, preferred_element_type=jnp.float32)).astype(jnp.bfloat16)
    return blocked_down(hidden, down_weight).astype(jnp.bfloat16)

def reference(queries, keys, values, cum_gate, head_gain, moe_in, ffn_gain, routes, route_weight, expert_gate, expert_up, expert_down, shared_gate, shared_up, shared_down):
    query_heads = queries.reshape(SEQ, HEADS, HEAD).transpose(1, 0, 2)
    key_heads = keys.reshape(SEQ, HEADS, HEAD).transpose(1, 0, 2)
    value_heads = values.reshape(SEQ, HEADS, HEAD).transpose(1, 0, 2)
    summed = lax.map(attend_head, (query_heads, key_heads, value_heads, cum_gate.T))
    mean_square = lax.optimization_barrier(jnp.mean(summed * summed, axis=2, keepdims=True))
    normed_heads = summed * lax.rsqrt(mean_square + NORM_EPSILON) * head_gain.reshape(HEADS, 1, HEAD)
    mixed = normed_heads.transpose(1, 0, 2).reshape(SEQ, QW).astype(jnp.bfloat16)
    source = moe_in.astype(jnp.float32)
    normed = (source * lax.rsqrt(lax.optimization_barrier(jnp.mean(source * source, axis=1, keepdims=True)) + NORM_EPSILON) * ffn_gain).astype(jnp.bfloat16)
    shared_hidden = (jax.nn.silu(jnp.dot(normed, shared_gate.T, preferred_element_type=jnp.float32)) * jnp.dot(normed, shared_up.T, preferred_element_type=jnp.float32)).astype(jnp.bfloat16)
    shared_sum = blocked_down(shared_hidden, shared_down)
    token_blocks = normed.reshape(N_EP, MROWS, D)
    route_blocks = routes.reshape(N_EP, MROWS, TOP)
    slot_ids = jax.vmap(slot_index)(route_blocks)
    buffers = jax.vmap(fill_slots)(token_blocks, slot_ids)
    by_expert = buffers.reshape(N_EP, EXPERTS, CAP, D).transpose(1, 0, 2, 3).reshape(EXPERTS, N_EP * CAP, D)
    results = lax.map(run_expert, (by_expert, expert_gate, expert_up, expert_down))
    returned = results.reshape(EXPERTS, N_EP, CAP, D).transpose(1, 0, 2, 3).reshape(N_EP, EXPERTS * CAP, D)
    picked = returned[jnp.arange(N_EP, dtype=jnp.int32)[:, None], slot_ids]
    picked = picked.reshape(MTOK, TOP, D).astype(jnp.float32)
    routed = lax.optimization_barrier(jnp.sum(picked * route_weight[:, :, None], axis=1))
    expert_out = (shared_sum + routed).astype(jnp.bfloat16)
    return (mixed, expert_out)
```

```python
import functools
import math

import jax
import jax.numpy as jnp
from jax import lax
from jax.experimental import pallas as pl
from jax.experimental.pallas import tpu as pltpu
from jax.sharding import PartitionSpec as P

NORM_EPSILON = 1e-06
VMEM = pltpu.VMEM


def swap_halves(x):
    half = x.shape[1] // 2
    return jnp.concatenate([x[:, half:], x[:, :half]], axis=1)


def pack_kernel(splits, scale, q_ref, k_ref, v_ref, kv_ref, qp_ref):
    rows, width = q_ref.shape
    tile = rows // splits
    half = tile // 2
    low = lax.broadcasted_iota(jnp.int32, (rows, 128), 1) < 64
    low_half = low[:half]
    for head in range(width // 64):
        lanes = slice(head // 2 * 128, head // 2 * 128 + 128)
        kc, vc = k_ref[:, lanes], v_ref[:, lanes]
        qc = q_ref[:, lanes] * jnp.asarray(scale, q_ref.dtype)
        if head % 2 == 0:
            kv_ref[head] = jnp.where(low, kc, swap_halves(vc))
        else:
            kv_ref[head] = jnp.where(low, swap_halves(kc), vc)
        for part in range(splits):
            a = qc[part * tile : part * tile + half]
            b = qc[part * tile + half : (part + 1) * tile]
            if head % 2 == 0:
                packed = jnp.where(low_half, a, swap_halves(b))
            else:
                packed = jnp.where(low_half, swap_halves(a), b)
            qp_ref[head * splits + part] = packed


def flash_kernel(splits, packed, key_len, q_ref, kv_ref, gate_ref, gain_ref, out_ref):
    block = pl.program_id(0)
    part = lax.rem(lax.axis_index("ep"), splits)
    raw = q_ref[0]
    half = raw.shape[0]
    if packed:
        low = lax.broadcasted_iota(jnp.int32, raw.shape, 1) < 64
        zero = jnp.zeros_like(raw)
        query = jnp.concatenate(
            [jnp.where(low, raw, zero), jnp.where(low, swap_halves(raw), zero)], axis=0
        )
    else:
        query = raw
    rows = query.shape[0]

    def visit(step, state, masked):
        peak, weighted = state
        keys = kv_ref[pl.ds(pl.multiple_of(step * key_len, key_len), key_len), :]
        scores = lax.dot_general(
            query, keys, (((1,), (1,)), ((), ())), preferred_element_type=jnp.float32
        )
        scores = scores - gate_ref[step]
        if masked:
            row_pos = part * rows + lax.broadcasted_iota(jnp.int32, scores.shape, 0)
            key_pos = lax.broadcasted_iota(jnp.int32, scores.shape, 1)
            scores = jnp.where(key_pos <= row_pos, scores, -jnp.inf)
        new_peak = jnp.maximum(peak, jnp.max(scores, axis=1, keepdims=True))
        weights = jnp.exp(scores - new_peak).astype(jnp.bfloat16)
        weighted = weighted * jnp.exp(peak - new_peak) + jnp.dot(
            weights, keys, preferred_element_type=jnp.float32
        )
        return new_peak, weighted

    state = (jnp.full((rows, 1), -1e30, jnp.float32), jnp.zeros((rows, 128), jnp.float32))
    state = visit(block, state, True)
    state = lax.fori_loop(0, block, lambda step, s: visit(step, s, False), state)
    _, weighted = state
    high = lax.broadcasted_iota(jnp.int32, weighted.shape, 1) >= 64
    square = jnp.sum(jnp.where(high, weighted * weighted, 0.0), axis=1, keepdims=True) / 64
    normed = weighted * lax.rsqrt(square + NORM_EPSILON) * gain_ref[...]
    if packed:
        normed = jnp.where(high[:half], normed[half:], swap_halves(normed[:half]))
    out_ref[0] = normed.astype(out_ref.dtype)


def trade_small(cum_gate, routes, route_weight):
    rows, heads = cum_gate.shape
    devices = lax.axis_size("ep")
    tokens, choose = routes.shape
    gates = jnp.repeat(cum_gate.T, devices // heads, axis=0)
    named = jnp.concatenate([routes.astype(jnp.float32).reshape(-1), route_weight.reshape(-1)])
    small = jnp.concatenate([gates, jnp.broadcast_to(named, (devices, named.size))], axis=1)
    small = lax.all_to_all(small, "ep", split_axis=0, concat_axis=0, tiled=True)
    count = tokens * choose
    all_routes = small[:, rows : rows + count].astype(jnp.int32).reshape(-1, choose)
    all_weights = small[:, rows + count :].reshape(-1, choose)
    return small[:, :rows], all_routes, all_weights


def trade_rows(queries, keys, values, heads):
    rows, width = queries.shape
    size = width // heads
    devices = lax.axis_size("ep")
    splits = devices // heads
    tile = rows // splits
    scale = size**-0.5
    packed = heads % 2 == 0 and (tile // 2) % 16 == 0
    send_rows = tile // 2 if packed else tile
    if packed:
        kv, qp = pl.pallas_call(
            functools.partial(pack_kernel, splits, scale),
            out_shape=(
                jax.ShapeDtypeStruct((heads, rows, 128), jnp.bfloat16),
                jax.ShapeDtypeStruct((devices, send_rows, 128), jnp.bfloat16),
            ),
            name="pack",
        )(queries, keys, values)
    else:
        kv = jnp.concatenate(
            [keys.reshape(rows, heads, size), values.reshape(rows, heads, size)], axis=2
        ).transpose(1, 0, 2)
        qs = (queries * jnp.asarray(scale, queries.dtype)).reshape(splits, tile, heads, size)
        qs = qs.transpose(2, 0, 1, 3).reshape(devices, tile, size)
        qp = jnp.concatenate([qs, jnp.zeros_like(qs)], axis=2)
    parcel = jnp.concatenate([jnp.repeat(kv, splits, axis=0), qp], axis=1)
    return lax.all_to_all(parcel, "ep", split_axis=0, concat_axis=0, tiled=True), packed


def attend(got, packed, rows, all_gates, heads, head_gain):
    devices, parcel_rows, _ = got.shape
    width = head_gain.shape[0]
    size = width // heads
    splits = devices // heads
    tile = rows // splits
    send_rows = parcel_rows - rows
    kv_all = got[:, :rows].reshape(devices * rows, 128)
    q_all = got[:, rows:]
    head = lax.axis_index("ep") // splits
    gain = lax.dynamic_slice_in_dim(head_gain, head * size, size, 0)
    gain = jnp.concatenate([gain, gain])[None]
    flops = 2 * 2 * 128 * devices * (devices + 1) // 2 * tile * rows
    out = pl.pallas_call(
        functools.partial(flash_kernel, splits, packed, rows),
        grid=(devices,),
        in_specs=[
            pl.BlockSpec((1, send_rows, 128), lambda i: (i, 0, 0)),
            pl.BlockSpec(memory_space=VMEM),
            pl.BlockSpec(memory_space=VMEM),
            pl.BlockSpec(memory_space=VMEM),
        ],
        out_specs=pl.BlockSpec((1, send_rows, 128), lambda i: (i, 0, 0)),
        out_shape=jax.ShapeDtypeStruct((devices, send_rows, 128), jnp.bfloat16),
        cost_estimate=pl.CostEstimate(
            flops=flops, bytes_accessed=4 * devices * rows * 128, transcendentals=flops // 512
        ),
        compiler_params=pltpu.CompilerParams(vmem_limit_bytes=40 << 20),
        name="flash",
    )(q_all, kv_all, all_gates.reshape(devices, 1, rows), gain)
    back = lax.all_to_all(out, "ep", split_axis=0, concat_axis=0, tiled=True)
    if packed:
        back = back.reshape(heads, splits, tile // 2, 2, size).transpose(1, 3, 2, 0, 4)
    else:
        back = back[:, :, size:].reshape(heads, splits, tile, size).transpose(1, 2, 0, 3)
    return back.reshape(rows, width)


def norm_kernel(x_ref, gain_ref, out_ref):
    parts, _, width = x_ref.shape
    pieces = [x_ref[part].astype(jnp.float32) for part in range(parts)]
    square = sum(jnp.sum(p * p, axis=1, keepdims=True) for p in pieces) / (parts * width)
    factor = lax.rsqrt(square + NORM_EPSILON)
    for part, piece in enumerate(pieces):
        lanes = slice(part * width, (part + 1) * width)
        out_ref[:, lanes] = (piece * factor * gain_ref[:, lanes]).astype(out_ref.dtype)


def gated(rows, gate, up):
    dims = (((1,), (1,)), ((), ()))
    gate_value = lax.dot_general(rows, gate, dims, preferred_element_type=jnp.float32)
    up_value = lax.dot_general(rows, up, dims, preferred_element_type=jnp.float32)
    return gate_value / (1.0 + jnp.exp(-gate_value)) * up_value


def hidden_kernel(
    x_ref, routes_ref, weight_ref, gate_ref, up_ref, sgate_ref, sup_ref, hid_ref, shid_ref
):
    expert = pl.program_id(0)
    here = lax.axis_index("ep")
    tokens = shid_ref.shape[0]
    number = here * pl.num_programs(0) + expert
    chunk = min(256, x_ref.shape[0])

    @pl.loop(0, x_ref.shape[0] // chunk)
    def _(step):
        rows = pl.ds(pl.multiple_of(step * chunk, chunk), chunk)
        share = jnp.sum(
            jnp.where(routes_ref[rows, :] == number, weight_ref[rows, :], 0.0),
            axis=1,
            keepdims=True,
        )
        value = gated(x_ref[rows, :], gate_ref[0], up_ref[0])
        hid_ref[0, rows, :] = (value * share).astype(hid_ref.dtype)

    @pl.when(expert == 0)
    def _():
        own = x_ref[pl.ds(pl.multiple_of(here * tokens, tokens), tokens), :]
        shid_ref[...] = gated(own, sgate_ref[...], sup_ref[...]).astype(shid_ref.dtype)


def down_kernel(hid_ref, shid_ref, down_ref, sdown_ref, out_ref):
    tokens = shid_ref.shape[0]
    here = lax.axis_index("ep")
    per_group = down_ref.shape[0]

    @pl.loop(0, hid_ref.shape[1] // tokens)
    def _(step):
        rows = pl.ds(pl.multiple_of(step * tokens, tokens), tokens)
        term = sum(
            jnp.dot(hid_ref[expert, rows, :], down_ref[expert], preferred_element_type=jnp.float32)
            for expert in range(per_group)
        )
        out_ref[0, rows, :] = term.astype(out_ref.dtype)

        @pl.when(step == here)
        def _():
            extra = jnp.dot(shid_ref[...], sdown_ref[...], preferred_element_type=jnp.float32)
            out_ref[0, rows, :] = (term + extra).astype(out_ref.dtype)


def gather_tokens(moe_in):
    slice_width = moe_in.shape[1] // lax.axis_size("tp")
    own_columns = lax.dynamic_slice_in_dim(
        moe_in, lax.axis_index("tp") * slice_width, slice_width, 1
    )
    return lax.all_gather(own_columns, ("ep", "tp"), axis=0)


def expert_terms(
    gathered,
    ffn_gain,
    all_routes,
    all_weights,
    expert_gate,
    expert_up,
    expert_down,
    shared_gate,
    shared_up,
    shared_down,
):
    tokens = gathered.shape[1]
    model_width = ffn_gain.shape[0]
    per_group, hidden_width = expert_gate.shape[:2]
    shared_width = shared_gate.shape[0]
    groups = lax.axis_size("ep")
    parts = lax.axis_size("tp")
    slice_width = model_width // parts
    total = groups * tokens
    params = pltpu.CompilerParams(vmem_limit_bytes=48 << 20)
    whole = pl.BlockSpec(memory_space=VMEM)
    normed = pl.pallas_call(
        norm_kernel,
        grid=(groups,),
        in_specs=[pl.BlockSpec((parts, tokens, slice_width), lambda i: (i, 0, 0)), whole],
        out_specs=pl.BlockSpec((tokens, model_width), lambda i: (i, 0)),
        out_shape=jax.ShapeDtypeStruct((total, model_width), jnp.bfloat16),
        cost_estimate=pl.CostEstimate(
            flops=4 * total * model_width, bytes_accessed=4 * total * model_width, transcendentals=0
        ),
        name="norm",
    )(gathered, ffn_gain[None])
    weight_spec = pl.BlockSpec((1, hidden_width, model_width), lambda i: (i, 0, 0))
    columns = per_group * hidden_width
    hidden, shared_hidden = pl.pallas_call(
        hidden_kernel,
        grid=(per_group,),
        in_specs=[whole, whole, whole, weight_spec, weight_spec, whole, whole],
        out_specs=(
            pl.BlockSpec((1, total, hidden_width), lambda i: (i, 0, 0)),
            pl.BlockSpec((tokens, shared_width), lambda i: (0, 0)),
        ),
        out_shape=(
            jax.ShapeDtypeStruct((per_group, total, hidden_width), jnp.bfloat16),
            jax.ShapeDtypeStruct((tokens, shared_width), jnp.bfloat16),
        ),
        cost_estimate=pl.CostEstimate(
            flops=4 * total * model_width * columns,
            bytes_accessed=4 * columns * model_width,
            transcendentals=total * columns,
        ),
        compiler_params=params,
        name="hidden",
    )(normed, all_routes, all_weights, expert_gate, expert_up, shared_gate, shared_up)
    return pl.pallas_call(
        down_kernel,
        grid=(parts,),
        in_specs=[
            whole,
            whole,
            pl.BlockSpec((per_group, hidden_width, slice_width), lambda i: (0, 0, i)),
            pl.BlockSpec((shared_width, slice_width), lambda i: (0, i)),
        ],
        out_specs=pl.BlockSpec((1, total, slice_width), lambda i: (i, 0, 0)),
        out_shape=jax.ShapeDtypeStruct((parts, total, slice_width), jnp.bfloat16),
        cost_estimate=pl.CostEstimate(
            flops=2 * total * model_width * columns,
            bytes_accessed=2 * (columns + total) * model_width,
            transcendentals=0,
        ),
        compiler_params=params,
        name="down",
    )(hidden, shared_hidden, expert_down, shared_down)


def combine_terms(term):
    groups = lax.axis_size("ep")
    _, total, slice_width = term.shape
    tokens = total // groups
    summed = lax.psum_scatter(term, "tp", scatter_dimension=0, tiled=True)
    back = lax.all_to_all(
        summed.reshape(groups, tokens, slice_width), "ep", split_axis=0, concat_axis=0, tiled=True
    )
    return jnp.sum(back.astype(jnp.float32), axis=0).astype(jnp.bfloat16)


MESH = pl.DeviceIdType.MESH
COPIES = 64


def flipped(number, mask, bits=3):
    total = 0
    for bit in range(bits):
        digit = lax.rem(number // (1 << bit), 2)
        total = total + ((1 - digit) if (mask >> bit) & 1 else digit) * (1 << bit)
    return total


def fused_kernel(
    cap,
    q_ref,
    k_ref,
    v_ref,
    small_ref,
    gain_ref,
    moe_ref,
    ffn_ref,
    egate_hbm,
    eup_hbm,
    edown_hbm,
    sgate_hbm,
    sup_hbm,
    sdown_hbm,
    mixed_ref,
    expert_ref,
    kvs,
    qs,
    kv_all,
    q_all,
    small_all,
    peak_buf,
    acc_buf,
    o_send,
    o_recv,
    x_all,
    xg,
    sel_buf,
    share_buf,
    egate,
    eup,
    edown,
    sgate,
    sup,
    sdown,
    y_buf,
    ysh,
    r1,
    r1s,
    s_send,
    ss_send,
    r2,
    r2s,
    term_buf,
    t_send,
    r3,
    u_send,
    r4,
    wsem,
    send_sem,
    recv_sem,
):
    e = lax.axis_index("ep")
    t = lax.axis_index("tp")
    z, x = e // 2, lax.rem(e, 2)
    y, c = t // 2, lax.rem(t, 2)
    ty = (1 - y) * 2 + c
    tc = y * 2 + 1 - c
    rows, width = q_ref.shape
    heads = width // 64
    tile = rows // 2
    half = tile // 2
    tokens, model = moe_ref.shape
    quarter = model // 4
    per_group, hid, _ = egate.shape
    slot2 = 2 * cap
    slots = per_group * slot2

    def peer(m):
        return flipped(e, m)

    def pair(k):
        return flipped(z, k, 2)

    ids = {}

    def remote(name, src, dst, device):
        n = ids.setdefault(name, len(ids))
        return pltpu.make_async_remote_copy(
            src_ref=src,
            dst_ref=dst,
            send_sem=send_sem.at[n],
            recv_sem=recv_sem.at[n],
            device_id=device,
            device_id_type=MESH,
        )

    def block(b, col, count=1):
        return x_all.at[
            pl.ds(pl.multiple_of(b * tokens, tokens), count * tokens),
            pl.ds(pl.multiple_of(col * quarter, quarter), quarter),
        ]

    def small(m):
        return remote(
            ("small", m), small_ref.at[pair(m // 2)], small_all.at[e], {"ep": peer(m)}
        )

    def gz(k):
        return remote(("gz", k), block(e, t), block(e, t), {"ep": peer(2 * k)})

    def gx(k):
        b = peer(2 * k)
        return remote(("gx", k), block(b, t), block(b, t), {"ep": peer(1)})

    def pair_rows(k, col):
        if k == 0:
            return block(peer(1), col)
        return block(pair(k) * 2, col, 2)

    def gy(k):
        return remote(("gy", k), pair_rows(k, t), pair_rows(k, t), {"tp": ty})

    def gd0(k):
        return remote(("gd0", k), pair_rows(k, t), pair_rows(k, t), {"tp": tc})

    def gd1(k):
        return remote(("gd1", k), pair_rows(k, ty), pair_rows(k, ty), {"tp": tc})

    def kvz(k):
        return remote(("kvz", k), kvs.at[pair(k)], kv_all.at[e], {"ep": peer(2 * k)})

    def kvx(k):
        b = peer(2 * k)
        return remote(("kvx", k), kv_all.at[b], kv_all.at[b], {"ep": peer(1)})

    def qc(m):
        part = (1 - x) if m % 2 else x
        return remote(("q", m), qs.at[pair(m // 2), part], q_all.at[e], {"ep": peer(m)})

    def c_r1(k):
        return remote(("r1", k), y_buf.at[1 - c, :, k], r1.at[:, k], {"tp": tc})

    def c_r1s():
        return remote("r1s", ysh.at[1 - c], r1s, {"tp": tc})

    def c_r2(k):
        return remote(("r2", k), s_send.at[k], r2.at[k], {"tp": ty})

    def c_r2s():
        return remote("r2s", ss_send, r2s, {"tp": ty})

    def c_r3(k):
        return remote(("r3", k), t_send.at[k], r3.at[k], {"ep": peer(1)})

    def c_r4(k):
        return remote(("r4", k), u_send.at[k], r4.at[k], {"ep": peer(2 * k)})

    def c_o(m):
        return remote(("o", m), o_send.at[peer(m)], o_recv.at[e], {"ep": peer(m)})

    started = []

    def start(copy_fn, *args):
        copy_fn(*args).start()
        started.append((copy_fn, args))

    barrier = pltpu.get_barrier_semaphore()
    for m in range(1, 8):
        pl.semaphore_signal(barrier, inc=1, device_id={"ep": peer(m)}, device_id_type=MESH)
    for other in (ty, tc):
        pl.semaphore_signal(barrier, inc=1, device_id={"tp": other}, device_id_type=MESH)

    loads = [
        pltpu.make_async_copy(src, dst, wsem.at[n])
        for n, (src, dst) in enumerate(
            (
                (sgate_hbm, sgate),
                (sup_hbm, sup),
                (sdown_hbm, sdown),
                (egate_hbm, egate),
                (eup_hbm, eup),
                (edown_hbm, edown),
            )
        )
    ]
    for load in loads:
        load.start()

    own = moe_ref[...].astype(jnp.float32)
    square = jnp.sum(own * own, axis=1, keepdims=True) / model
    own = (own * lax.rsqrt(square + NORM_EPSILON) * ffn_ref[...]).astype(jnp.bfloat16)
    own_rows = pl.ds(pl.multiple_of(e * tokens, tokens), tokens)
    x_all[own_rows, :] = own
    small_all[e] = small_ref[z]

    pl.semaphore_wait(barrier, 9)
    for k in (1, 2, 3):
        start(gz, k)
    start(gx, 0)
    for m in range(1, 8):
        start(small, m)

    low = lax.broadcasted_iota(jnp.int32, (rows, 128), 1) < 64
    low_half = low[:half]
    for head in range(heads):
        lanes = slice(head // 2 * 128, head // 2 * 128 + 128)
        kc, vc = k_ref[:, lanes], v_ref[:, lanes]
        qq = q_ref[:, lanes] * jnp.asarray(0.125, q_ref.dtype)
        if head % 2 == 0:
            kvs[head] = jnp.where(low, kc, swap_halves(vc))
        else:
            kvs[head] = jnp.where(low, swap_halves(kc), vc)
        for part in range(2):
            a = qq[part * tile : part * tile + half]
            b = qq[part * tile + half : (part + 1) * tile]
            if head % 2 == 0:
                packed = jnp.where(low_half, a, swap_halves(b))
            else:
                packed = jnp.where(low_half, swap_halves(a), b)
            qs[head, part] = packed
    kv_all[e] = kvs[z]
    q_all[e] = qs[z, x]
    start(kvx, 0)
    start(qc, 1)
    for k in (1, 2, 3):
        start(kvz, k)
        start(qc, 2 * k)
        start(qc, 2 * k + 1)

    peak_buf[...] = jnp.full(peak_buf.shape, -1e30, jnp.float32)
    acc_buf[...] = jnp.zeros(acc_buf.shape, jnp.float32)

    low_q = low_half
    high = lax.broadcasted_iota(jnp.int32, (tile, 128), 1) >= 64

    def visit(i, j, masked):
        raw = q_all[i]
        zero = jnp.zeros_like(raw)
        query = jnp.concatenate(
            [jnp.where(low_q, raw, zero), jnp.where(low_q, swap_halves(raw), zero)], axis=0
        )
        keys = kv_all[j]
        scores = lax.dot_general(
            query, keys, (((1,), (1,)), ((), ())), preferred_element_type=jnp.float32
        )
        gates = jnp.concatenate(
            [small_all[j, 8 + r : 9 + r, :] for r in range(rows // 128)], axis=1
        )
        scores = scores - gates
        if masked:
            row_pos = x * tile + lax.broadcasted_iota(jnp.int32, scores.shape, 0)
            key_pos = lax.broadcasted_iota(jnp.int32, scores.shape, 1)
            scores = jnp.where(key_pos <= row_pos, scores, -jnp.inf)
        peak = peak_buf[i]
        new_peak = jnp.maximum(peak, jnp.max(scores, axis=1, keepdims=True))
        weights = jnp.exp(scores - new_peak).astype(jnp.bfloat16)
        acc_buf[i] = acc_buf[i] * jnp.exp(peak - new_peak) + jnp.dot(
            weights, keys, preferred_element_type=jnp.float32
        )
        peak_buf[i] = new_peak

    def diagonal(k):
        pk = pair(k)

        @pl.loop(0, 2)
        def _(v):
            visit(2 * pk + v, 2 * pk + v, True)

    def visits(k, first, last, events=None):
        pk = pair(k)

        @pl.loop(first, last)
        def _(v):
            inner = (v + 63) // 64
            u = v + 1 - inner - inner
            m = u // 4 + (1 - inner) * 0
            pm = 0
            for bit in range(2):
                digit = lax.rem(lax.rem(z // (1 << bit), 2) + lax.rem(m // (1 << bit), 2), 2)
                pm = pm + digit * (1 << bit)
            above = (pk - pm + 4) // 4
            hi = pm + above * (pk - pm)
            lo = pk - above * (pk - pm)
            i = inner * (2 * hi + lax.rem(u // 2, 2)) + (1 - inner) * (2 * pk + 1)
            j = inner * (2 * lo + lax.rem(u, 2)) + (1 - inner) * (2 * pk)
            visit(i, j, False)
            for at, event in (events or {}).items():
                pl.when(v == at)(event)

    def epilogue(k):
        for xx in range(2):
            m = 2 * k + xx
            i = peer(m)
            weighted = acc_buf[i]
            square = jnp.sum(jnp.where(high, weighted * weighted, 0.0), axis=1, keepdims=True) / 64
            out = weighted * lax.rsqrt(square + NORM_EPSILON) * gain_ref[z]
            out = jnp.where(high[:half], out[half:], swap_halves(out[:half]))
            out = out.astype(o_send.dtype)
            if m == 0:
                o_recv[e] = out
            else:
                o_send[i] = out
                start(c_o, m)

    upper = (
        lax.broadcasted_iota(jnp.int32, (tokens, tokens), 0)
        <= lax.broadcasted_iota(jnp.int32, (tokens, tokens), 1)
    )
    upper = jnp.where(upper, 1.0, 0.0).astype(jnp.bfloat16)

    def select(k):
        pk = pair(k)
        named, chosen = [], []
        for bb in range(2):
            table = small_all[2 * pk + bb]
            ids_of = table[0:4].astype(jnp.int32)
            share = table[4:8]
            for j in range(per_group):
                hit = ids_of == e * per_group + j
                named.append(jnp.sum(jnp.where(hit, 1.0, 0.0), axis=0, keepdims=True))
                chosen.append(jnp.sum(jnp.where(hit, share, 0.0), axis=0, keepdims=True))
        flags = jnp.concatenate(named, axis=0)
        rank = jnp.dot(flags.astype(jnp.bfloat16), upper, preferred_element_type=jnp.float32)
        slot = jnp.where(flags > 0.5, rank - 1.0, -1000.0)
        row_of = lax.broadcasted_iota(jnp.int32, (slot2, 2 * tokens), 0).astype(jnp.float32)
        for j in range(per_group):
            target = jnp.concatenate(
                [slot[j : j + 1], slot[per_group + j : per_group + j + 1] + float(cap)], axis=1
            )
            share = jnp.concatenate([chosen[j], chosen[per_group + j]], axis=1)
            match = row_of == target
            sel_buf[k, j * slot2 : (j + 1) * slot2, :] = jnp.where(match, 1.0, 0.0).astype(
                jnp.bfloat16
            )
            share_buf[j, k * slot2 : (k + 1) * slot2, :] = jnp.sum(
                jnp.where(match, share, 0.0), axis=1, keepdims=True
            )

    def pick(k):
        gd0(k).wait_recv()
        gd1(k).wait_recv()
        pair_at = pl.ds(pl.multiple_of(pair(k) * 2 * tokens, 2 * tokens), 2 * tokens)
        for part in range(4):
            cols = slice(part * quarter, (part + 1) * quarter)
            picked = jnp.dot(
                sel_buf[k], x_all[pair_at, cols], preferred_element_type=jnp.float32
            ).astype(jnp.bfloat16)
            for j in range(per_group):
                xg[j, k * slot2 : (k + 1) * slot2, cols] = picked[j * slot2 : (j + 1) * slot2]

    def e1(k):
        gz(k).wait_recv()
        start(gx, k)

    def e2(k):
        gx(k).wait_recv()
        start(gy, k)
        start(gd0, k)

    def e3(k):
        gy(k).wait_recv()
        start(gd1, k)

    def forward(k):
        kvz(k).wait_recv()
        start(kvx, k)

    def ready(k):
        kvx(k).wait_recv()
        for m in (2 * k, 2 * k + 1):
            if m:
                qc(m).wait_recv()

    for load in loads[:3]:
        load.wait()
    shared_hidden = gated(x_all[own_rows, :], sgate[...], sup[...]).astype(jnp.bfloat16)
    for part in range(4):
        cols = slice(part * quarter, (part + 1) * quarter)
        ysh[part % 2, part // 2] = jnp.dot(
            shared_hidden, sdown[:, cols], preferred_element_type=jnp.float32
        ).astype(jnp.bfloat16)
    e2(0)
    e1(1)
    e2(1)
    for m in range(1, 8):
        small(m).wait_recv()
    for k in range(4):
        select(k)
    e1(2)
    e3(0)
    e2(2)
    e1(3)
    e2(3)
    ready(0)
    diagonal(0)
    visits(0, 0, 1)
    e3(1)
    pick(0)
    forward(1)
    pick(1)
    e3(2)
    ready(1)
    diagonal(1)
    visits(1, 0, 5)
    e3(3)
    pick(2)
    forward(2)
    pick(3)
    for load in loads[3:]:
        load.wait()

    @pl.loop(0, per_group)
    def _(j):
        value = gated(xg[j], egate[j], eup[j])
        hidden = (value * share_buf[j]).astype(jnp.bfloat16)
        at = pl.ds(pl.multiple_of(j * slot2, 16), slot2)
        for part in range(4):
            cols = slice(part * quarter, (part + 1) * quarter)
            out = jnp.dot(
                hidden, edown[j, :, cols], preferred_element_type=jnp.float32
            ).astype(jnp.bfloat16)
            for k in range(4):
                y_buf[part % 2, part // 2, k, at, :] = out[k * slot2 : (k + 1) * slot2]

    for k in (3, 2, 1, 0):
        start(c_r1, k)
    start(c_r1s)

    def wide(ref):
        return ref.astype(jnp.float32)

    def core_sum(k):
        c_r1(k).wait_recv()
        s_send[k] = (wide(y_buf[c, 1 - y, k]) + wide(r1[1 - y, k])).astype(jnp.bfloat16)
        c_r2(k).start()

    def shared_sum():
        c_r1s().wait_recv()
        ss_send[...] = (wide(ysh[c, 1 - y]) + wide(r1s[1 - y])).astype(jnp.bfloat16)
        c_r2s().start()

    def scatter(k):
        c_r2(k).wait_recv()
        total = wide(y_buf[c, y, k]) + wide(r1[y, k]) + wide(r2[k])
        term = lax.dot_general(
            sel_buf[k],
            total.astype(jnp.bfloat16),
            (((0,), (0,)), ((), ())),
            preferred_element_type=jnp.float32,
        )
        term_buf[k, 0] = term[:tokens]
        term_buf[k, 1] = term[tokens:]
        t_send[k] = term_buf[k, 1 - x].astype(jnp.bfloat16)
        c_r3(k).start()

    def combine(k):
        c_r3(k).wait_recv()
        u_send[k] = (term_buf[k, x] + wide(r3[k])).astype(jnp.bfloat16)
        c_r4(k).start()

    for k in range(4):
        started.append((c_r2, (k,)))
        started.append((c_r3, (k,)))
        if k:
            started.append((c_r4, (k,)))
    started.append((c_r2s, ()))

    forward(3)
    core_sum(3)
    core_sum(2)
    ready(2)
    diagonal(2)
    core_sum(1)
    core_sum(0)
    shared_sum()
    visits(2, 0, 9)
    scatter(3)
    ready(3)
    diagonal(3)
    visits(3, 0, 5)
    epilogue(0)
    combine(3)
    scatter(2)
    visits(3, 5, 9)
    epilogue(1)
    combine(2)
    scatter(1)
    visits(3, 9, 13)
    epilogue(2)
    epilogue(3)
    combine(1)
    scatter(0)
    c_r2s().wait_recv()
    c_r3(0).wait_recv()
    out = term_buf[0, x] + wide(r3[0]) + wide(ysh[c, y]) + wide(r1s[y]) + wide(r2s[...])
    for k in (3, 2, 1):
        c_r4(k).wait_recv()
        out = out + wide(r4[k])
    expert_ref[...] = out.astype(expert_ref.dtype)

    for m in range(1, 8):
        c_o(m).wait_recv()
    for part in range(2):
        for head in range(0, heads, 2):
            lanes = slice(head // 2 * 128, head // 2 * 128 + 128)
            first, second = o_recv[head * 2 + part], o_recv[(head + 1) * 2 + part]
            at = part * tile
            mixed_ref[at : at + half, lanes] = jnp.where(low_half, first, swap_halves(second))
            mixed_ref[at + half : at + tile, lanes] = jnp.where(
                low_half, swap_halves(first), second
            )
    for copy_fn, args in started:
        copy_fn(*args).wait_send()


def fused(
    queries,
    keys,
    values,
    cum_gate,
    head_gain,
    moe_in,
    ffn_gain,
    routes,
    route_weight,
    expert_gate,
    expert_up,
    expert_down,
    shared_gate,
    shared_up,
    shared_down,
):
    rows, heads = cum_gate.shape
    width = queries.shape[1]
    tokens, model = moe_in.shape
    choose = routes.shape[1]
    per_group, hid, _ = expert_gate.shape
    experts = per_group * lax.axis_size("ep")
    cap = 3 * tokens * choose // (2 * experts)
    devices = lax.axis_size("ep")
    tile, half, quarter = rows // 2, rows // 4, model // 4
    slots = per_group * 2 * cap
    shared = shared_gate.shape[0]
    lines = rows // 128
    gates = cum_gate.T.reshape(heads, lines, 128)
    named = jnp.concatenate([routes.astype(jnp.float32), route_weight], axis=1).T
    small = jnp.concatenate(
        [
            jnp.broadcast_to(named, (heads, 2 * choose, 128)),
            gates,
            jnp.zeros((heads, 8 - lines, 128), jnp.float32),
        ],
        axis=1,
    )
    gain = head_gain.reshape(heads, 1, 64)
    gain = jnp.concatenate([gain, gain], axis=2)
    bf16, f32 = jnp.bfloat16, jnp.float32
    vmem = pl.BlockSpec(memory_space=VMEM)
    hbm = pl.BlockSpec(memory_space=pl.ANY)
    scratch = [
        VMEM((heads, rows, 128), bf16),
        VMEM((heads, 2, half, 128), bf16),
        VMEM((devices, rows, 128), bf16),
        VMEM((devices, half, 128), bf16),
        VMEM((devices, 16, 128), f32),
        VMEM((devices, tile, 1), f32),
        VMEM((devices, tile, 128), f32),
        VMEM((devices, half, 128), bf16),
        VMEM((devices, half, 128), bf16),
        VMEM((devices * tokens, model), bf16),
        VMEM((per_group, 8 * cap, model), bf16),
        VMEM((4, slots, 2 * tokens), bf16),
        VMEM((per_group, 8 * cap, 1), f32),
        VMEM((per_group, hid, model), bf16),
        VMEM((per_group, hid, model), bf16),
        VMEM((per_group, hid, model), bf16),
        VMEM((shared, model), bf16),
        VMEM((shared, model), bf16),
        VMEM((shared, model), bf16),
        VMEM((2, 2, 4, slots, quarter), bf16),
        VMEM((2, 2, tokens, quarter), bf16),
        VMEM((2, 4, slots, quarter), bf16),
        VMEM((2, tokens, quarter), bf16),
        VMEM((4, slots, quarter), bf16),
        VMEM((tokens, quarter), bf16),
        VMEM((4, slots, quarter), bf16),
        VMEM((tokens, quarter), bf16),
        VMEM((4, 2, tokens, quarter), f32),
        VMEM((4, tokens, quarter), bf16),
        VMEM((4, tokens, quarter), bf16),
        VMEM((4, tokens, quarter), bf16),
        VMEM((4, tokens, quarter), bf16),
        pltpu.SemaphoreType.DMA((6,)),
        pltpu.SemaphoreType.DMA((COPIES,)),
        pltpu.SemaphoreType.DMA((COPIES,)),
    ]
    return pl.pallas_call(
        functools.partial(fused_kernel, cap),
        in_specs=[vmem] * 7 + [hbm] * 6,
        out_specs=(vmem, vmem),
        out_shape=(
            jax.ShapeDtypeStruct((rows, width), bf16),
            jax.ShapeDtypeStruct((tokens, quarter), bf16),
        ),
        scratch_shapes=scratch,
        compiler_params=pltpu.CompilerParams(
            collective_id=0, has_side_effects=True, vmem_limit_bytes=62 << 20
        ),
        name="fused",
    )(
        queries,
        keys,
        values,
        small,
        gain,
        moe_in,
        ffn_gain[None],
        expert_gate,
        expert_up,
        expert_down,
        shared_gate,
        shared_up,
        shared_down,
    )


def fits_fused(cum_gate, queries, moe_in, routes, expert_gate):
    rows, heads = cum_gate.shape
    tokens, choose = routes.shape
    per_group = expert_gate.shape[0]
    devices = lax.axis_size("ep")
    cap = 3 * tokens * choose // (2 * per_group * devices)
    return (
        devices == 8
        and lax.axis_size("tp") == 4
        and heads == 4
        and queries.shape[1] == 256
        and rows % 128 == 0
        and rows // 128 <= 8
        and (rows // 4) % 16 == 0
        and tokens == 128
        and choose == 4
        and per_group == 4
        and (2 * cap) % 16 == 0
    )


def on_device(
    queries,
    keys,
    values,
    cum_gate,
    head_gain,
    moe_in,
    ffn_gain,
    routes,
    route_weight,
    expert_gate,
    expert_up,
    expert_down,
    shared_gate,
    shared_up,
    shared_down,
):
    if fits_fused(cum_gate, queries, moe_in, routes, expert_gate):
        return fused(
            queries,
            keys,
            values,
            cum_gate,
            head_gain,
            moe_in,
            ffn_gain,
            routes,
            route_weight,
            expert_gate,
            expert_up,
            expert_down,
            shared_gate,
            shared_up,
            shared_down,
        )
    rows, heads = cum_gate.shape
    gathered = gather_tokens(moe_in)
    got, packed = trade_rows(queries, keys, values, heads)
    all_gates, all_routes, all_weights = trade_small(cum_gate, routes, route_weight)
    gathered, got = lax.optimization_barrier((gathered, got))
    term = expert_terms(
        gathered,
        ffn_gain,
        all_routes,
        all_weights,
        expert_gate,
        expert_up,
        expert_down,
        shared_gate,
        shared_up,
        shared_down,
    )
    term, got = lax.optimization_barrier((term, got))
    mixed = attend(got, packed, rows, all_gates, heads, head_gain)
    return (mixed, combine_terms(term))


def solution(mesh):
    in_specs = (
        P("ep", "tp"),
        P("ep", "tp"),
        P("ep", "tp"),
        P("ep", "tp"),
        P("tp"),
        P("ep", None),
        P(),
        P("ep", None),
        P("ep", None),
        P("ep", "tp", None),
        P("ep", "tp", None),
        P("ep", "tp", None),
        P("tp", None),
        P("tp", None),
        P("tp", None),
    )
    out_specs = (P("ep", "tp"), P("ep", "tp"))
    return jax.shard_map(
        on_device, mesh=mesh, in_specs=in_specs, out_specs=out_specs, check_vma=False
    )
```

```python
import functools
import math

import jax
import jax.numpy as jnp
from jax import lax
from jax.experimental import pallas as pl
from jax.experimental.pallas import tpu as pltpu
from jax.sharding import PartitionSpec as P

NORM_EPSILON = 1e-06
VMEM = pltpu.VMEM


def swap_halves(x):
    half = x.shape[1] // 2
    return jnp.concatenate([x[:, half:], x[:, :half]], axis=1)


def pack_kernel(splits, scale, q_ref, k_ref, v_ref, kv_ref, qp_ref):
    rows, width = q_ref.shape
    tile = rows // splits
    half = tile // 2
    low = lax.broadcasted_iota(jnp.int32, (rows, 128), 1) < 64
    low_half = low[:half]
    for head in range(width // 64):
        lanes = slice(head // 2 * 128, head // 2 * 128 + 128)
        kc, vc = k_ref[:, lanes], v_ref[:, lanes]
        qc = q_ref[:, lanes] * jnp.asarray(scale, q_ref.dtype)
        if head % 2 == 0:
            kv_ref[head] = jnp.where(low, kc, swap_halves(vc))
        else:
            kv_ref[head] = jnp.where(low, swap_halves(kc), vc)
        for part in range(splits):
            a = qc[part * tile : part * tile + half]
            b = qc[part * tile + half : (part + 1) * tile]
            if head % 2 == 0:
                packed = jnp.where(low_half, a, swap_halves(b))
            else:
                packed = jnp.where(low_half, swap_halves(a), b)
            qp_ref[head * splits + part] = packed


def flash_kernel(splits, packed, key_len, q_ref, kv_ref, gate_ref, gain_ref, out_ref):
    block = pl.program_id(0)
    part = lax.rem(lax.axis_index("ep"), splits)
    raw = q_ref[0]
    half = raw.shape[0]
    if packed:
        low = lax.broadcasted_iota(jnp.int32, raw.shape, 1) < 64
        zero = jnp.zeros_like(raw)
        query = jnp.concatenate(
            [jnp.where(low, raw, zero), jnp.where(low, swap_halves(raw), zero)], axis=0
        )
    else:
        query = raw
    rows = query.shape[0]

    def visit(step, state, masked):
        peak, weighted = state
        keys = kv_ref[pl.ds(pl.multiple_of(step * key_len, key_len), key_len), :]
        scores = lax.dot_general(
            query, keys, (((1,), (1,)), ((), ())), preferred_element_type=jnp.float32
        )
        scores = scores - gate_ref[step]
        if masked:
            row_pos = part * rows + lax.broadcasted_iota(jnp.int32, scores.shape, 0)
            key_pos = lax.broadcasted_iota(jnp.int32, scores.shape, 1)
            scores = jnp.where(key_pos <= row_pos, scores, -jnp.inf)
        new_peak = jnp.maximum(peak, jnp.max(scores, axis=1, keepdims=True))
        weights = jnp.exp(scores - new_peak).astype(jnp.bfloat16)
        weighted = weighted * jnp.exp(peak - new_peak) + jnp.dot(
            weights, keys, preferred_element_type=jnp.float32
        )
        return new_peak, weighted

    state = (jnp.full((rows, 1), -1e30, jnp.float32), jnp.zeros((rows, 128), jnp.float32))
    state = visit(block, state, True)
    state = lax.fori_loop(0, block, lambda step, s: visit(step, s, False), state)
    _, weighted = state
    high = lax.broadcasted_iota(jnp.int32, weighted.shape, 1) >= 64
    square = jnp.sum(jnp.where(high, weighted * weighted, 0.0), axis=1, keepdims=True) / 64
    normed = weighted * lax.rsqrt(square + NORM_EPSILON) * gain_ref[...]
    if packed:
        normed = jnp.where(high[:half], normed[half:], swap_halves(normed[:half]))
    out_ref[0] = normed.astype(out_ref.dtype)


def trade_small(cum_gate, routes, route_weight):
    rows, heads = cum_gate.shape
    devices = lax.axis_size("ep")
    tokens, choose = routes.shape
    gates = jnp.repeat(cum_gate.T, devices // heads, axis=0)
    named = jnp.concatenate([routes.astype(jnp.float32).reshape(-1), route_weight.reshape(-1)])
    small = jnp.concatenate([gates, jnp.broadcast_to(named, (devices, named.size))], axis=1)
    small = lax.all_to_all(small, "ep", split_axis=0, concat_axis=0, tiled=True)
    count = tokens * choose
    all_routes = small[:, rows : rows + count].astype(jnp.int32).reshape(-1, choose)
    all_weights = small[:, rows + count :].reshape(-1, choose)
    return small[:, :rows], all_routes, all_weights


def trade_rows(queries, keys, values, heads):
    rows, width = queries.shape
    size = width // heads
    devices = lax.axis_size("ep")
    splits = devices // heads
    tile = rows // splits
    scale = size**-0.5
    packed = heads % 2 == 0 and (tile // 2) % 16 == 0
    send_rows = tile // 2 if packed else tile
    if packed:
        kv, qp = pl.pallas_call(
            functools.partial(pack_kernel, splits, scale),
            out_shape=(
                jax.ShapeDtypeStruct((heads, rows, 128), jnp.bfloat16),
                jax.ShapeDtypeStruct((devices, send_rows, 128), jnp.bfloat16),
            ),
            name="pack",
        )(queries, keys, values)
    else:
        kv = jnp.concatenate(
            [keys.reshape(rows, heads, size), values.reshape(rows, heads, size)], axis=2
        ).transpose(1, 0, 2)
        qs = (queries * jnp.asarray(scale, queries.dtype)).reshape(splits, tile, heads, size)
        qs = qs.transpose(2, 0, 1, 3).reshape(devices, tile, size)
        qp = jnp.concatenate([qs, jnp.zeros_like(qs)], axis=2)
    parcel = jnp.concatenate([jnp.repeat(kv, splits, axis=0), qp], axis=1)
    return lax.all_to_all(parcel, "ep", split_axis=0, concat_axis=0, tiled=True), packed


def attend(got, packed, rows, all_gates, heads, head_gain):
    devices, parcel_rows, _ = got.shape
    width = head_gain.shape[0]
    size = width // heads
    splits = devices // heads
    tile = rows // splits
    send_rows = parcel_rows - rows
    kv_all = got[:, :rows].reshape(devices * rows, 128)
    q_all = got[:, rows:]
    head = lax.axis_index("ep") // splits
    gain = lax.dynamic_slice_in_dim(head_gain, head * size, size, 0)
    gain = jnp.concatenate([gain, gain])[None]
    flops = 2 * 2 * 128 * devices * (devices + 1) // 2 * tile * rows
    out = pl.pallas_call(
        functools.partial(flash_kernel, splits, packed, rows),
        grid=(devices,),
        in_specs=[
            pl.BlockSpec((1, send_rows, 128), lambda i: (i, 0, 0)),
            pl.BlockSpec(memory_space=VMEM),
            pl.BlockSpec(memory_space=VMEM),
            pl.BlockSpec(memory_space=VMEM),
        ],
        out_specs=pl.BlockSpec((1, send_rows, 128), lambda i: (i, 0, 0)),
        out_shape=jax.ShapeDtypeStruct((devices, send_rows, 128), jnp.bfloat16),
        cost_estimate=pl.CostEstimate(
            flops=flops, bytes_accessed=4 * devices * rows * 128, transcendentals=flops // 512
        ),
        compiler_params=pltpu.CompilerParams(vmem_limit_bytes=40 << 20),
        name="flash",
    )(q_all, kv_all, all_gates.reshape(devices, 1, rows), gain)
    back = lax.all_to_all(out, "ep", split_axis=0, concat_axis=0, tiled=True)
    if packed:
        back = back.reshape(heads, splits, tile // 2, 2, size).transpose(1, 3, 2, 0, 4)
    else:
        back = back[:, :, size:].reshape(heads, splits, tile, size).transpose(1, 2, 0, 3)
    return back.reshape(rows, width)


def norm_kernel(x_ref, gain_ref, out_ref):
    parts, _, width = x_ref.shape
    pieces = [x_ref[part].astype(jnp.float32) for part in range(parts)]
    square = sum(jnp.sum(p * p, axis=1, keepdims=True) for p in pieces) / (parts * width)
    factor = lax.rsqrt(square + NORM_EPSILON)
    for part, piece in enumerate(pieces):
        lanes = slice(part * width, (part + 1) * width)
        out_ref[:, lanes] = (piece * factor * gain_ref[:, lanes]).astype(out_ref.dtype)


def gated(rows, gate, up):
    dims = (((1,), (1,)), ((), ()))
    gate_value = lax.dot_general(rows, gate, dims, preferred_element_type=jnp.float32)
    up_value = lax.dot_general(rows, up, dims, preferred_element_type=jnp.float32)
    return gate_value / (1.0 + jnp.exp(-gate_value)) * up_value


def hidden_kernel(
    x_ref, routes_ref, weight_ref, gate_ref, up_ref, sgate_ref, sup_ref, hid_ref, shid_ref
):
    expert = pl.program_id(0)
    here = lax.axis_index("ep")
    tokens = shid_ref.shape[0]
    number = here * pl.num_programs(0) + expert
    chunk = min(256, x_ref.shape[0])

    @pl.loop(0, x_ref.shape[0] // chunk)
    def _(step):
        rows = pl.ds(pl.multiple_of(step * chunk, chunk), chunk)
        share = jnp.sum(
            jnp.where(routes_ref[rows, :] == number, weight_ref[rows, :], 0.0),
            axis=1,
            keepdims=True,
        )
        value = gated(x_ref[rows, :], gate_ref[0], up_ref[0])
        hid_ref[0, rows, :] = (value * share).astype(hid_ref.dtype)

    @pl.when(expert == 0)
    def _():
        own = x_ref[pl.ds(pl.multiple_of(here * tokens, tokens), tokens), :]
        shid_ref[...] = gated(own, sgate_ref[...], sup_ref[...]).astype(shid_ref.dtype)


def down_kernel(hid_ref, shid_ref, down_ref, sdown_ref, out_ref):
    tokens = shid_ref.shape[0]
    here = lax.axis_index("ep")
    per_group = down_ref.shape[0]

    @pl.loop(0, hid_ref.shape[1] // tokens)
    def _(step):
        rows = pl.ds(pl.multiple_of(step * tokens, tokens), tokens)
        term = sum(
            jnp.dot(hid_ref[expert, rows, :], down_ref[expert], preferred_element_type=jnp.float32)
            for expert in range(per_group)
        )
        out_ref[0, rows, :] = term.astype(out_ref.dtype)

        @pl.when(step == here)
        def _():
            extra = jnp.dot(shid_ref[...], sdown_ref[...], preferred_element_type=jnp.float32)
            out_ref[0, rows, :] = (term + extra).astype(out_ref.dtype)


def gather_tokens(moe_in):
    slice_width = moe_in.shape[1] // lax.axis_size("tp")
    own_columns = lax.dynamic_slice_in_dim(
        moe_in, lax.axis_index("tp") * slice_width, slice_width, 1
    )
    return lax.all_gather(own_columns, ("ep", "tp"), axis=0)


def expert_terms(
    gathered,
    ffn_gain,
    all_routes,
    all_weights,
    expert_gate,
    expert_up,
    expert_down,
    shared_gate,
    shared_up,
    shared_down,
):
    tokens = gathered.shape[1]
    model_width = ffn_gain.shape[0]
    per_group, hidden_width = expert_gate.shape[:2]
    shared_width = shared_gate.shape[0]
    groups = lax.axis_size("ep")
    parts = lax.axis_size("tp")
    slice_width = model_width // parts
    total = groups * tokens
    params = pltpu.CompilerParams(vmem_limit_bytes=48 << 20)
    whole = pl.BlockSpec(memory_space=VMEM)
    normed = pl.pallas_call(
        norm_kernel,
        grid=(groups,),
        in_specs=[pl.BlockSpec((parts, tokens, slice_width), lambda i: (i, 0, 0)), whole],
        out_specs=pl.BlockSpec((tokens, model_width), lambda i: (i, 0)),
        out_shape=jax.ShapeDtypeStruct((total, model_width), jnp.bfloat16),
        cost_estimate=pl.CostEstimate(
            flops=4 * total * model_width, bytes_accessed=4 * total * model_width, transcendentals=0
        ),
        name="norm",
    )(gathered, ffn_gain[None])
    weight_spec = pl.BlockSpec((1, hidden_width, model_width), lambda i: (i, 0, 0))
    columns = per_group * hidden_width
    hidden, shared_hidden = pl.pallas_call(
        hidden_kernel,
        grid=(per_group,),
        in_specs=[whole, whole, whole, weight_spec, weight_spec, whole, whole],
        out_specs=(
            pl.BlockSpec((1, total, hidden_width), lambda i: (i, 0, 0)),
            pl.BlockSpec((tokens, shared_width), lambda i: (0, 0)),
        ),
        out_shape=(
            jax.ShapeDtypeStruct((per_group, total, hidden_width), jnp.bfloat16),
            jax.ShapeDtypeStruct((tokens, shared_width), jnp.bfloat16),
        ),
        cost_estimate=pl.CostEstimate(
            flops=4 * total * model_width * columns,
            bytes_accessed=4 * columns * model_width,
            transcendentals=total * columns,
        ),
        compiler_params=params,
        name="hidden",
    )(normed, all_routes, all_weights, expert_gate, expert_up, shared_gate, shared_up)
    return pl.pallas_call(
        down_kernel,
        grid=(parts,),
        in_specs=[
            whole,
            whole,
            pl.BlockSpec((per_group, hidden_width, slice_width), lambda i: (0, 0, i)),
            pl.BlockSpec((shared_width, slice_width), lambda i: (0, i)),
        ],
        out_specs=pl.BlockSpec((1, total, slice_width), lambda i: (i, 0, 0)),
        out_shape=jax.ShapeDtypeStruct((parts, total, slice_width), jnp.bfloat16),
        cost_estimate=pl.CostEstimate(
            flops=2 * total * model_width * columns,
            bytes_accessed=2 * (columns + total) * model_width,
            transcendentals=0,
        ),
        compiler_params=params,
        name="down",
    )(hidden, shared_hidden, expert_down, shared_down)


def combine_terms(term):
    groups = lax.axis_size("ep")
    _, total, slice_width = term.shape
    tokens = total // groups
    summed = lax.psum_scatter(term, "tp", scatter_dimension=0, tiled=True)
    back = lax.all_to_all(
        summed.reshape(groups, tokens, slice_width), "ep", split_axis=0, concat_axis=0, tiled=True
    )
    return jnp.sum(back.astype(jnp.float32), axis=0).astype(jnp.bfloat16)


MESH = pl.DeviceIdType.MESH
COPIES = 64
LOG2E = math.log2(math.e)


def flipped(number, mask, bits=3):
    total = 0
    for bit in range(bits):
        digit = lax.rem(number // (1 << bit), 2)
        total = total + ((1 - digit) if (mask >> bit) & 1 else digit) * (1 << bit)
    return total


def fused_kernel(
    cap,
    q_ref,
    k_ref,
    v_ref,
    cum_ref,
    routes_ref,
    weight_ref,
    gain_ref,
    moe_ref,
    ffn_ref,
    egate_hbm,
    eup_hbm,
    edown_hbm,
    sgate_hbm,
    sup_hbm,
    sdown_hbm,
    mixed_ref,
    expert_ref,
    small_ref,
    kvs,
    qs,
    kv_all,
    q_all,
    kg,
    vt,
    qx,
    small_all,
    peak_buf,
    acc_buf,
    o_send,
    o_recv,
    x_all,
    xg,
    sel_buf,
    share_buf,
    egate,
    eup,
    edown,
    sgate,
    sup,
    sdown,
    y_buf,
    ysh,
    r1,
    r1s,
    s_send,
    ss_send,
    r2,
    r2s,
    term_buf,
    t_send,
    r3,
    u_send,
    r4,
    wsem,
    send_sem,
    recv_sem,
):
    e = lax.axis_index("ep")
    t = lax.axis_index("tp")
    z, x = e // 2, lax.rem(e, 2)
    y, c = t // 2, lax.rem(t, 2)
    ty = (1 - y) * 2 + c
    tc = y * 2 + 1 - c
    rows, width = q_ref.shape
    heads = width // 64
    tile = rows // 2
    half = tile // 2
    tokens, model = moe_ref.shape
    quarter = model // 4
    per_group, hid, _ = egate.shape
    slot2 = 2 * cap
    slots = per_group * slot2

    def peer(m):
        return flipped(e, m)

    def pair(k):
        return flipped(z, k, 2)

    ids = {}

    def remote(name, src, dst, device):
        n = ids.setdefault(name, len(ids))
        return pltpu.make_async_remote_copy(
            src_ref=src,
            dst_ref=dst,
            send_sem=send_sem.at[n],
            recv_sem=recv_sem.at[n],
            device_id=device,
            device_id_type=MESH,
        )

    def block(b, col, count=1):
        return x_all.at[
            pl.ds(pl.multiple_of(b * tokens, tokens), count * tokens),
            pl.ds(pl.multiple_of(col * quarter, quarter), quarter),
        ]

    def small(m):
        return remote(
            ("small", m), small_ref.at[pair(m // 2)], small_all.at[e], {"ep": peer(m)}
        )

    def gz(k):
        b, to = (peer(4), peer(2)) if k == 3 else (e, peer(2 * k))
        return remote(("gz", k), block(b, t), block(b, t), {"ep": to})

    def gx(k):
        b = peer(2 * k)
        return remote(("gx", k), block(b, t), block(b, t), {"ep": peer(1)})

    def pair_rows(k, col):
        if k == 0:
            return block(peer(1), col)
        return block(pair(k) * 2, col, 2)

    def gy(k):
        return remote(("gy", k), pair_rows(k, t), pair_rows(k, t), {"tp": ty})

    def gd0(k):
        return remote(("gd0", k), pair_rows(k, t), pair_rows(k, t), {"tp": tc})

    def gd1(k):
        return remote(("gd1", k), pair_rows(k, ty), pair_rows(k, ty), {"tp": tc})

    def kvz(k):
        return remote(("kvz", k), kvs.at[pair(k)], kv_all.at[e], {"ep": peer(2 * k)})

    def kvx(k):
        b = peer(2 * k)
        return remote(("kvx", k), kv_all.at[b], kv_all.at[b], {"ep": peer(1)})

    def qc(m):
        part = (1 - x) if m % 2 else x
        return remote(("q", m), qs.at[pair(m // 2), part], q_all.at[e], {"ep": peer(m)})

    def c_r1(k):
        return remote(("r1", k), y_buf.at[1 - c, :, k], r1.at[:, k], {"tp": tc})

    def c_r1s():
        return remote("r1s", ysh.at[1 - c], r1s, {"tp": tc})

    def c_r2(k):
        return remote(("r2", k), s_send.at[k], r2.at[k], {"tp": ty})

    def c_r2s():
        return remote("r2s", ss_send, r2s, {"tp": ty})

    def c_r3(k):
        return remote(("r3", k), t_send.at[k], r3.at[k], {"ep": peer(1)})

    def c_r4(k):
        to = peer(2) if k == 3 else peer(2 * k)
        return remote(("r4", k), u_send.at[k], r4.at[k], {"ep": to})

    def c_o(m):
        return remote(("o", m), o_send.at[peer(m)], o_recv.at[e], {"ep": peer(m)})

    started = []

    def start(copy_fn, *args):
        copy_fn(*args).start()
        started.append((copy_fn, args))

    barrier = pltpu.get_barrier_semaphore()
    for m in range(1, 8):
        pl.semaphore_signal(barrier, inc=1, device_id={"ep": peer(m)}, device_id_type=MESH)
    for other in (ty, tc):
        pl.semaphore_signal(barrier, inc=1, device_id={"tp": other}, device_id_type=MESH)

    loads = [
        pltpu.make_async_copy(src, dst, wsem.at[n])
        for n, (src, dst) in enumerate(
            (
                (sgate_hbm, sgate),
                (sup_hbm, sup),
                (sdown_hbm, sdown),
                (egate_hbm, egate),
                (eup_hbm, eup),
                (edown_hbm, edown),
            )
        )
    ]
    for load in loads:
        load.start()

    own = moe_ref[...].astype(jnp.float32)
    square = jnp.sum(own * own, axis=1, keepdims=True) / model
    own = (own * lax.rsqrt(square + NORM_EPSILON) * ffn_ref[...]).astype(jnp.bfloat16)
    own_rows = pl.ds(pl.multiple_of(e * tokens, tokens), tokens)
    x_all[own_rows, :] = own

    lines = rows // 128
    for head in range(heads):
        small_ref[head, 0:4, :] = routes_ref[...].astype(jnp.float32)
        small_ref[head, 4:8, :] = weight_ref[...]
        small_ref[head, 8:16, :] = jnp.concatenate(
            [cum_ref[head : head + 1, r * 128 : (r + 1) * 128] for r in range(lines)]
            + [jnp.zeros((8 - lines, 128), jnp.float32)],
            axis=0,
        )
    small_all[e] = small_ref[z]

    low = lax.broadcasted_iota(jnp.int32, (rows, 128), 1) < 64
    low_half = low[:half]
    for head in range(heads):
        lanes = slice(head // 2 * 128, head // 2 * 128 + 128)
        kc, vc = k_ref[:, lanes], v_ref[:, lanes]
        qq = q_ref[:, lanes]
        if head % 2 == 0:
            kvs[head] = jnp.where(low, kc, swap_halves(vc))
        else:
            kvs[head] = jnp.where(low, swap_halves(kc), vc)
        for part in range(2):
            a = qq[part * tile : part * tile + half]
            b = qq[part * tile + half : (part + 1) * tile]
            if head % 2 == 0:
                packed = jnp.where(low_half, a, swap_halves(b))
            else:
                packed = jnp.where(low_half, swap_halves(a), b)
            qs[head, part] = packed
    kv_all[e] = kvs[z]
    q_all[e] = qs[z, x]
    pl.semaphore_wait(barrier, 9)
    for m in (7, 6, 5, 4, 3, 2, 1):
        start(small, m)
    start(gz, 1)
    start(gz, 2)
    start(gx, 0)

    lane = lax.broadcasted_iota(jnp.int32, (1, 128), 1)
    spread = jnp.where(
        lax.broadcasted_iota(jnp.int32, (16, 128), 0) + 64
        == lax.broadcasted_iota(jnp.int32, (16, 128), 1),
        1.0,
        0.0,
    )
    gate_lane = lax.broadcasted_iota(jnp.int32, (16, 128), 0) < 3
    spread = jnp.where(gate_lane, spread, 0.0).astype(jnp.bfloat16)
    pick_value = jnp.where(
        lax.broadcasted_iota(jnp.int32, (64, 128), 0) + 64
        == lax.broadcasted_iota(jnp.int32, (64, 128), 1),
        1.0,
        0.0,
    ).astype(jnp.bfloat16)
    unit = jnp.where(lane < 67, 1.0, 0.0).astype(jnp.bfloat16)
    both = (((1,), (1,)), ((), ()))

    def prep_kv(j):
        kv = kv_all[j]
        left = small_all[j, 8:16, :] * -LOG2E
        split = []
        for _ in range(3):
            piece = left.astype(jnp.bfloat16).astype(jnp.float32)
            split.append(jnp.concatenate([piece[r : r + 1] for r in range(lines)], axis=1))
            left = left - piece
        split.append(jnp.zeros((13, rows), jnp.float32))
        split = jnp.concatenate(split, axis=0).astype(jnp.bfloat16)
        gates = lax.dot_general(
            split, spread, (((0,), (0,)), ((), ())), preferred_element_type=jnp.float32
        )
        kg[j] = jnp.where(low, kv, gates.astype(jnp.bfloat16))
        vt[j] = lax.dot_general(
            pick_value, kv, both, preferred_element_type=jnp.float32
        ).astype(jnp.bfloat16)

    def prep_q(i):
        raw = q_all[i].astype(jnp.float32) * (LOG2E * 64**-0.5)
        first = raw.astype(jnp.bfloat16)
        second = (raw - first.astype(jnp.float32)).astype(jnp.bfloat16)
        zero = jnp.zeros_like(first)
        for n, (value, rest) in enumerate(((first, zero), (second, zero + unit))):
            qx[i, :, n * 128 : (n + 1) * 128] = jnp.concatenate(
                [jnp.where(low_half, value, rest), jnp.where(low_half, swap_halves(value), rest)],
                axis=0,
            )

    def scores_of(j, query):
        keys = jnp.concatenate([kv_all[j], kg[j]], axis=1)
        return lax.dot_general(keys, query, both, preferred_element_type=jnp.float32)

    def update(j, scores, peak, out):
        new_peak = jnp.maximum(peak, jnp.max(scores, axis=0, keepdims=True))
        weights = jnp.exp2(scores - new_peak).astype(jnp.bfloat16)
        out = out * jnp.exp2(peak - new_peak) + jnp.dot(
            vt[j], weights, preferred_element_type=jnp.float32
        )
        return new_peak, out

    def diagonal(k):
        pk = pair(k)
        first, second = qx[2 * pk], qx[2 * pk + 1]
        query = jnp.concatenate([first, second], axis=0)
        scores = scores_of(2 * pk, query)
        later = scores_of(2 * pk + 1, second)
        key_pos = lax.broadcasted_iota(jnp.int32, (rows, 2 * tile), 0)
        row_pos = lax.broadcasted_iota(jnp.int32, (rows, 2 * tile), 1)
        allowed = (key_pos <= row_pos + x * tile) | (row_pos >= tile)
        scores = jnp.where(allowed, scores, -jnp.inf)
        peak = jnp.max(scores, axis=0, keepdims=True)
        weights = jnp.exp2(scores - peak).astype(jnp.bfloat16)
        out = jnp.dot(vt[2 * pk], weights, preferred_element_type=jnp.float32)
        key_pos = lax.broadcasted_iota(jnp.int32, (rows, tile), 0)
        row_pos = lax.broadcasted_iota(jnp.int32, (rows, tile), 1)
        later = jnp.where(key_pos <= row_pos + x * tile, later, -jnp.inf)
        last_peak, last_out = update(2 * pk + 1, later, peak[:, tile:], out[:, tile:])
        peak_buf[pk, :, :tile] = peak[:, :tile]
        peak_buf[pk, :, tile:] = last_peak
        acc_buf[pk, :, :tile] = out[:, :tile]
        acc_buf[pk, :, tile:] = last_out

    def cross(k, m):
        pk, pm = pair(k), pair(m)
        above = (pk - pm + 4) // 4
        hi = pm + above * (pk - pm)
        lo = pk - above * (pk - pm)
        query = jnp.concatenate([qx[2 * hi], qx[2 * hi + 1]], axis=0)
        scores = scores_of(2 * lo, query)
        later = scores_of(2 * lo + 1, query)
        peak, out = update(2 * lo, scores, peak_buf[hi], acc_buf[hi])
        peak, out = update(2 * lo + 1, later, peak, out)
        peak_buf[hi] = peak
        acc_buf[hi] = out

    gain_pair = jnp.where(z // 2 == 0, gain_ref[:, :128], gain_ref[:, 128:])
    gain_swap = swap_halves(gain_pair)
    gain = jnp.where((lane < 64) == (lax.rem(z, 2) == 0), gain_pair, gain_swap)

    def epilogue(k):
        weighted = acc_buf[pair(k)]
        square = jnp.sum(weighted * weighted, axis=0, keepdims=True) / 64
        normed = weighted * lax.rsqrt(square + NORM_EPSILON)
        for xx in range(2):
            at = xx * tile
            out = jnp.concatenate(
                [normed[:, at : at + half], normed[:, at + half : at + tile]], axis=0
            ).T
            o_send[2 * pair(k) + xx] = (out * gain).astype(o_send.dtype)
        for m in (2 * k, 2 * k + 1):
            if m == 0:
                o_recv[e] = o_send[e]
            else:
                start(c_o, m)

    upper = (
        lax.broadcasted_iota(jnp.int32, (tokens, tokens), 0)
        <= lax.broadcasted_iota(jnp.int32, (tokens, tokens), 1)
    )
    upper = jnp.where(upper, 1.0, 0.0).astype(jnp.bfloat16)

    def select(k):
        pk = pair(k)
        named, chosen = [], []
        for bb in range(2):
            table = small_all[2 * pk + bb]
            ids_of = table[0:4].astype(jnp.int32)
            share = table[4:8]
            for j in range(per_group):
                hit = ids_of == e * per_group + j
                named.append(jnp.sum(jnp.where(hit, 1.0, 0.0), axis=0, keepdims=True))
                chosen.append(jnp.sum(jnp.where(hit, share, 0.0), axis=0, keepdims=True))
        flags = jnp.concatenate(named, axis=0)
        rank = jnp.dot(flags.astype(jnp.bfloat16), upper, preferred_element_type=jnp.float32)
        slot = jnp.where(flags > 0.5, rank - 1.0, -1000.0)
        row_of = lax.broadcasted_iota(jnp.int32, (slot2, 2 * tokens), 0).astype(jnp.float32)
        for j in range(per_group):
            target = jnp.concatenate(
                [slot[j : j + 1], slot[per_group + j : per_group + j + 1] + float(cap)], axis=1
            )
            share = jnp.concatenate([chosen[j], chosen[per_group + j]], axis=1)
            match = row_of == target
            sel_buf[k, j * slot2 : (j + 1) * slot2, :] = jnp.where(match, 1.0, 0.0).astype(
                jnp.bfloat16
            )
            share_buf[j, k * slot2 : (k + 1) * slot2, :] = jnp.sum(
                jnp.where(match, share, 0.0), axis=1, keepdims=True
            )

    def pick(k):
        gd0(k).wait_recv()
        gd1(k).wait_recv()
        pair_at = pl.ds(pl.multiple_of(pair(k) * 2 * tokens, 2 * tokens), 2 * tokens)
        for part in range(4):
            cols = slice(part * quarter, (part + 1) * quarter)
            picked = jnp.dot(
                sel_buf[k], x_all[pair_at, cols], preferred_element_type=jnp.float32
            ).astype(jnp.bfloat16)
            for j in range(per_group):
                xg[j, k * slot2 : (k + 1) * slot2, cols] = picked[j * slot2 : (j + 1) * slot2]

    def e1(k):
        gz(k).wait_recv()
        start(gx, k)

    def e2(k):
        gx(k).wait_recv()
        start(gy, k)
        start(gd0, k)

    def e3(k):
        gy(k).wait_recv()
        start(gd1, k)

    def forward(k):
        kvz(k).wait_recv()
        start(kvx, k)

    def ready(k):
        kvx(k).wait_recv()
        for m in (2 * k, 2 * k + 1):
            if m:
                qc(m).wait_recv()
            prep_kv(peer(m))
            prep_q(peer(m))

    for load in loads[:3]:
        load.wait()
    shared_hidden = gated(x_all[own_rows, :], sgate[...], sup[...]).astype(jnp.bfloat16)
    for part in range(4):
        cols = slice(part * quarter, (part + 1) * quarter)
        ysh[part % 2, part // 2] = jnp.dot(
            shared_hidden, sdown[:, cols], preferred_element_type=jnp.float32
        ).astype(jnp.bfloat16)
    def experts_of(chunk):
        span = 2 * slot2

        @pl.loop(0, per_group)
        def _(j):
            here = slice(chunk * span, (chunk + 1) * span)
            value = gated(xg[j, here, :], egate[j], eup[j])
            hidden = (value * share_buf[j, here, :]).astype(jnp.bfloat16)
            at = pl.ds(pl.multiple_of(j * slot2, 16), slot2)
            for part in range(4):
                cols = slice(part * quarter, (part + 1) * quarter)
                out = jnp.dot(
                    hidden, edown[j, :, cols], preferred_element_type=jnp.float32
                ).astype(jnp.bfloat16)
                for k in range(2):
                    y_buf[part % 2, part // 2, 2 * chunk + k, at, :] = out[
                        k * slot2 : (k + 1) * slot2
                    ]

    def wide(ref):
        return ref.astype(jnp.float32)

    def core_sum(k):
        c_r1(k).wait_recv()
        s_send[k] = (wide(y_buf[c, 1 - y, k]) + wide(r1[1 - y, k])).astype(jnp.bfloat16)
        c_r2(k).start()

    def shared_sum():
        c_r1s().wait_recv()
        ss_send[...] = (wide(ysh[c, 1 - y]) + wide(r1s[1 - y])).astype(jnp.bfloat16)
        c_r2s().start()

    def scatter(k):
        c_r2(k).wait_recv()
        total = wide(y_buf[c, y, k]) + wide(r1[y, k]) + wide(r2[k])
        term = lax.dot_general(
            sel_buf[k],
            total.astype(jnp.bfloat16),
            (((0,), (0,)), ((), ())),
            preferred_element_type=jnp.float32,
        )
        term_buf[k, 0] = term[:tokens]
        term_buf[k, 1] = term[tokens:]
        t_send[k] = term_buf[k, 1 - x].astype(jnp.bfloat16)
        c_r3(k).start()

    def combine(k):
        c_r3(k).wait_recv()
        total = term_buf[k, x] + wide(r3[k])
        if k == 2:
            c_r4(3).wait_recv()
            total = total + wide(r4[3])
        u_send[k] = total.astype(jnp.bfloat16)
        c_r4(k).start()

    for k in range(4):
        started.append((c_r2, (k,)))
        started.append((c_r3, (k,)))
        if k:
            started.append((c_r4, (k,)))
    started.append((c_r2s, ()))

    e2(0)
    e1(1)
    start(kvx, 0)
    start(qc, 1)
    for m in range(1, 8):
        small(m).wait_recv()
    for k in range(4):
        select(k)
    e3(0)
    e1(2)
    start(gz, 3)
    for k in (3, 2, 1):
        start(kvz, k)
        start(qc, 2 * k)
        start(qc, 2 * k + 1)
    e2(1)
    ready(0)
    pick(0)
    e2(2)
    diagonal(0)
    e1(3)
    e3(1)
    pick(1)
    for load in loads[3:]:
        load.wait()
    experts_of(0)
    start(c_r1, 1)
    start(c_r1, 0)
    start(c_r1s)
    e2(3)
    forward(3)
    core_sum(1)
    core_sum(0)
    shared_sum()
    e3(2)
    pick(2)
    ready(3)
    forward(2)
    diagonal(3)
    e3(3)
    pick(3)
    experts_of(1)
    start(c_r1, 3)
    start(c_r1, 2)
    forward(1)
    cross(3, 0)
    core_sum(3)
    core_sum(2)
    scatter(1)
    scatter(0)
    ready(2)
    diagonal(2)
    cross(2, 0)
    combine(1)
    cross(2, 3)
    scatter(3)
    ready(1)
    diagonal(1)
    scatter(2)
    cross(1, 3)
    epilogue(3)
    combine(3)
    cross(1, 2)
    epilogue(2)
    combine(2)
    cross(1, 0)
    epilogue(1)
    epilogue(0)
    c_r2s().wait_recv()
    c_r3(0).wait_recv()
    out = term_buf[0, x] + wide(r3[0]) + wide(ysh[c, y]) + wide(r1s[y]) + wide(r2s[...])
    for k in (2, 1):
        c_r4(k).wait_recv()
        out = out + wide(r4[k])
    expert_ref[...] = out.astype(expert_ref.dtype)

    for m in range(1, 8):
        c_o(m).wait_recv()
    mixed_ref[...] = o_recv[...]
    for copy_fn, args in started:
        copy_fn(*args).wait_send()


def finish_kernel(parcels_ref, sum_ref, mixed_ref, expert_ref):
    count, half, _ = parcels_ref.shape
    low_half = lax.broadcasted_iota(jnp.int32, (half, 128), 1) < 64
    for part in range(2):
        for head in range(0, count // 2, 2):
            lanes = slice(head // 2 * 128, head // 2 * 128 + 128)
            first, second = parcels_ref[head * 2 + part], parcels_ref[(head + 1) * 2 + part]
            at = part * 2 * half
            mixed_ref[at : at + half, lanes] = jnp.where(low_half, first, swap_halves(second))
            mixed_ref[at + half : at + 2 * half, lanes] = jnp.where(
                low_half, swap_halves(first), second
            )
    expert_ref[...] = sum_ref[...]


def fused(
    queries,
    keys,
    values,
    cum_gate,
    head_gain,
    moe_in,
    ffn_gain,
    routes,
    route_weight,
    expert_gate,
    expert_up,
    expert_down,
    shared_gate,
    shared_up,
    shared_down,
):
    rows, heads = cum_gate.shape
    width = queries.shape[1]
    tokens, model = moe_in.shape
    choose = routes.shape[1]
    per_group, hid, _ = expert_gate.shape
    experts = per_group * lax.axis_size("ep")
    cap = 3 * tokens * choose // (2 * experts)
    devices = lax.axis_size("ep")
    tile, half, quarter = rows // 2, rows // 4, model // 4
    slots = per_group * 2 * cap
    shared = shared_gate.shape[0]
    bf16, f32 = jnp.bfloat16, jnp.float32
    vmem = pl.BlockSpec(memory_space=VMEM)
    hbm = pl.BlockSpec(memory_space=pl.ANY)
    scratch = [
        VMEM((heads, 16, 128), f32),
        VMEM((heads, rows, 128), bf16),
        VMEM((heads, 2, half, 128), bf16),
        VMEM((devices, rows, 128), bf16),
        VMEM((devices, half, 128), bf16),
        VMEM((devices, rows, 128), bf16),
        VMEM((devices, 64, rows), bf16),
        VMEM((devices, tile, 256), bf16),
        VMEM((devices, 16, 128), f32),
        VMEM((4, 1, 2 * tile), f32),
        VMEM((4, 64, 2 * tile), f32),
        VMEM((devices, half, 128), bf16),
        VMEM((devices, half, 128), bf16),
        VMEM((devices * tokens, model), bf16),
        VMEM((per_group, 8 * cap, model), bf16),
        VMEM((4, slots, 2 * tokens), bf16),
        VMEM((per_group, 8 * cap, 1), f32),
        VMEM((per_group, hid, model), bf16),
        VMEM((per_group, hid, model), bf16),
        VMEM((per_group, hid, model), bf16),
        VMEM((shared, model), bf16),
        VMEM((shared, model), bf16),
        VMEM((shared, model), bf16),
        VMEM((2, 2, 4, slots, quarter), bf16),
        VMEM((2, 2, tokens, quarter), bf16),
        VMEM((2, 4, slots, quarter), bf16),
        VMEM((2, tokens, quarter), bf16),
        VMEM((4, slots, quarter), bf16),
        VMEM((tokens, quarter), bf16),
        VMEM((4, slots, quarter), bf16),
        VMEM((tokens, quarter), bf16),
        VMEM((4, 2, tokens, quarter), f32),
        VMEM((4, tokens, quarter), bf16),
        VMEM((4, tokens, quarter), bf16),
        VMEM((4, tokens, quarter), bf16),
        VMEM((4, tokens, quarter), bf16),
        pltpu.SemaphoreType.DMA((6,)),
        pltpu.SemaphoreType.DMA((COPIES,)),
        pltpu.SemaphoreType.DMA((COPIES,)),
    ]
    parcels, total = pl.pallas_call(
        functools.partial(fused_kernel, cap),
        in_specs=[vmem] * 9 + [hbm] * 6,
        out_specs=(vmem, vmem),
        out_shape=(
            jax.ShapeDtypeStruct((devices, half, 128), bf16),
            jax.ShapeDtypeStruct((tokens, quarter), bf16),
        ),
        scratch_shapes=scratch,
        compiler_params=pltpu.CompilerParams(
            collective_id=0, has_side_effects=True, vmem_limit_bytes=62 << 20
        ),
        name="fused",
    )(
        queries,
        keys,
        values,
        cum_gate.T,
        routes.T,
        route_weight.T,
        head_gain[None],
        moe_in,
        ffn_gain[None],
        expert_gate,
        expert_up,
        expert_down,
        shared_gate,
        shared_up,
        shared_down,
    )
    return pl.pallas_call(
        finish_kernel,
        in_specs=[vmem, vmem],
        out_specs=(vmem, vmem),
        out_shape=(
            jax.ShapeDtypeStruct((rows, width), bf16),
            jax.ShapeDtypeStruct((tokens, quarter), bf16),
        ),
        name="finish",
    )(parcels, total)


def fits_fused(cum_gate, queries, moe_in, routes, expert_gate):
    rows, heads = cum_gate.shape
    tokens, choose = routes.shape
    per_group = expert_gate.shape[0]
    devices = lax.axis_size("ep")
    cap = 3 * tokens * choose // (2 * per_group * devices)
    return (
        devices == 8
        and lax.axis_size("tp") == 4
        and heads == 4
        and queries.shape[1] == 256
        and rows % 128 == 0
        and rows // 128 <= 8
        and (rows // 4) % 16 == 0
        and tokens == 128
        and choose == 4
        and per_group == 4
        and (2 * cap) % 16 == 0
    )


def on_device(
    queries,
    keys,
    values,
    cum_gate,
    head_gain,
    moe_in,
    ffn_gain,
    routes,
    route_weight,
    expert_gate,
    expert_up,
    expert_down,
    shared_gate,
    shared_up,
    shared_down,
):
    if fits_fused(cum_gate, queries, moe_in, routes, expert_gate):
        return fused(
            queries,
            keys,
            values,
            cum_gate,
            head_gain,
            moe_in,
            ffn_gain,
            routes,
            route_weight,
            expert_gate,
            expert_up,
            expert_down,
            shared_gate,
            shared_up,
            shared_down,
        )
    rows, heads = cum_gate.shape
    gathered = gather_tokens(moe_in)
    got, packed = trade_rows(queries, keys, values, heads)
    all_gates, all_routes, all_weights = trade_small(cum_gate, routes, route_weight)
    gathered, got = lax.optimization_barrier((gathered, got))
    term = expert_terms(
        gathered,
        ffn_gain,
        all_routes,
        all_weights,
        expert_gate,
        expert_up,
        expert_down,
        shared_gate,
        shared_up,
        shared_down,
    )
    term, got = lax.optimization_barrier((term, got))
    mixed = attend(got, packed, rows, all_gates, heads, head_gain)
    return (mixed, combine_terms(term))


def solution(mesh):
    in_specs = (
        P("ep", "tp"),
        P("ep", "tp"),
        P("ep", "tp"),
        P("ep", "tp"),
        P("tp"),
        P("ep", None),
        P(),
        P("ep", None),
        P("ep", None),
        P("ep", "tp", None),
        P("ep", "tp", None),
        P("ep", "tp", None),
        P("tp", None),
        P("tp", None),
        P("tp", None),
    )
    out_specs = (P("ep", "tp"), P("ep", "tp"))
    return jax.shard_map(
        on_device, mesh=mesh, in_specs=in_specs, out_specs=out_specs, check_vma=False
    )
```

```python
import functools
import math

import jax
import jax.numpy as jnp
from jax import lax
from jax.experimental import pallas as pl
from jax.experimental.pallas import tpu as pltpu
from jax.sharding import PartitionSpec as P

NORM_EPSILON = 1e-06
VMEM = pltpu.VMEM


def swap_halves(x):
    half = x.shape[1] // 2
    return jnp.concatenate([x[:, half:], x[:, :half]], axis=1)


def pack_kernel(splits, scale, q_ref, k_ref, v_ref, kv_ref, qp_ref):
    rows, width = q_ref.shape
    tile = rows // splits
    half = tile // 2
    low = lax.broadcasted_iota(jnp.int32, (rows, 128), 1) < 64
    low_half = low[:half]
    for head in range(width // 64):
        lanes = slice(head // 2 * 128, head // 2 * 128 + 128)
        kc, vc = k_ref[:, lanes], v_ref[:, lanes]
        qc = q_ref[:, lanes] * jnp.asarray(scale, q_ref.dtype)
        if head % 2 == 0:
            kv_ref[head] = jnp.where(low, kc, swap_halves(vc))
        else:
            kv_ref[head] = jnp.where(low, swap_halves(kc), vc)
        for part in range(splits):
            a = qc[part * tile : part * tile + half]
            b = qc[part * tile + half : (part + 1) * tile]
            if head % 2 == 0:
                packed = jnp.where(low_half, a, swap_halves(b))
            else:
                packed = jnp.where(low_half, swap_halves(a), b)
            qp_ref[head * splits + part] = packed


def flash_kernel(splits, packed, key_len, q_ref, kv_ref, gate_ref, gain_ref, out_ref):
    block = pl.program_id(0)
    part = lax.rem(lax.axis_index("ep"), splits)
    raw = q_ref[0]
    half = raw.shape[0]
    if packed:
        low = lax.broadcasted_iota(jnp.int32, raw.shape, 1) < 64
        zero = jnp.zeros_like(raw)
        query = jnp.concatenate(
            [jnp.where(low, raw, zero), jnp.where(low, swap_halves(raw), zero)], axis=0
        )
    else:
        query = raw
    rows = query.shape[0]

    def visit(step, state, masked):
        peak, weighted = state
        keys = kv_ref[pl.ds(pl.multiple_of(step * key_len, key_len), key_len), :]
        scores = lax.dot_general(
            query, keys, (((1,), (1,)), ((), ())), preferred_element_type=jnp.float32
        )
        scores = scores - gate_ref[step]
        if masked:
            row_pos = part * rows + lax.broadcasted_iota(jnp.int32, scores.shape, 0)
            key_pos = lax.broadcasted_iota(jnp.int32, scores.shape, 1)
            scores = jnp.where(key_pos <= row_pos, scores, -jnp.inf)
        new_peak = jnp.maximum(peak, jnp.max(scores, axis=1, keepdims=True))
        weights = jnp.exp(scores - new_peak).astype(jnp.bfloat16)
        weighted = weighted * jnp.exp(peak - new_peak) + jnp.dot(
            weights, keys, preferred_element_type=jnp.float32
        )
        return new_peak, weighted

    state = (jnp.full((rows, 1), -1e30, jnp.float32), jnp.zeros((rows, 128), jnp.float32))
    state = visit(block, state, True)
    state = lax.fori_loop(0, block, lambda step, s: visit(step, s, False), state)
    _, weighted = state
    high = lax.broadcasted_iota(jnp.int32, weighted.shape, 1) >= 64
    square = jnp.sum(jnp.where(high, weighted * weighted, 0.0), axis=1, keepdims=True) / 64
    normed = weighted * lax.rsqrt(square + NORM_EPSILON) * gain_ref[...]
    if packed:
        normed = jnp.where(high[:half], normed[half:], swap_halves(normed[:half]))
    out_ref[0] = normed.astype(out_ref.dtype)


def trade_small(cum_gate, routes, route_weight):
    rows, heads = cum_gate.shape
    devices = lax.axis_size("ep")
    tokens, choose = routes.shape
    gates = jnp.repeat(cum_gate.T, devices // heads, axis=0)
    named = jnp.concatenate([routes.astype(jnp.float32).reshape(-1), route_weight.reshape(-1)])
    small = jnp.concatenate([gates, jnp.broadcast_to(named, (devices, named.size))], axis=1)
    small = lax.all_to_all(small, "ep", split_axis=0, concat_axis=0, tiled=True)
    count = tokens * choose
    all_routes = small[:, rows : rows + count].astype(jnp.int32).reshape(-1, choose)
    all_weights = small[:, rows + count :].reshape(-1, choose)
    return small[:, :rows], all_routes, all_weights


def trade_rows(queries, keys, values, heads):
    rows, width = queries.shape
    size = width // heads
    devices = lax.axis_size("ep")
    splits = devices // heads
    tile = rows // splits
    scale = size**-0.5
    packed = heads % 2 == 0 and (tile // 2) % 16 == 0
    send_rows = tile // 2 if packed else tile
    if packed:
        kv, qp = pl.pallas_call(
            functools.partial(pack_kernel, splits, scale),
            out_shape=(
                jax.ShapeDtypeStruct((heads, rows, 128), jnp.bfloat16),
                jax.ShapeDtypeStruct((devices, send_rows, 128), jnp.bfloat16),
            ),
            name="pack",
        )(queries, keys, values)
    else:
        kv = jnp.concatenate(
            [keys.reshape(rows, heads, size), values.reshape(rows, heads, size)], axis=2
        ).transpose(1, 0, 2)
        qs = (queries * jnp.asarray(scale, queries.dtype)).reshape(splits, tile, heads, size)
        qs = qs.transpose(2, 0, 1, 3).reshape(devices, tile, size)
        qp = jnp.concatenate([qs, jnp.zeros_like(qs)], axis=2)
    parcel = jnp.concatenate([jnp.repeat(kv, splits, axis=0), qp], axis=1)
    return lax.all_to_all(parcel, "ep", split_axis=0, concat_axis=0, tiled=True), packed


def attend(got, packed, rows, all_gates, heads, head_gain):
    devices, parcel_rows, _ = got.shape
    width = head_gain.shape[0]
    size = width // heads
    splits = devices // heads
    tile = rows // splits
    send_rows = parcel_rows - rows
    kv_all = got[:, :rows].reshape(devices * rows, 128)
    q_all = got[:, rows:]
    head = lax.axis_index("ep") // splits
    gain = lax.dynamic_slice_in_dim(head_gain, head * size, size, 0)
    gain = jnp.concatenate([gain, gain])[None]
    flops = 2 * 2 * 128 * devices * (devices + 1) // 2 * tile * rows
    out = pl.pallas_call(
        functools.partial(flash_kernel, splits, packed, rows),
        grid=(devices,),
        in_specs=[
            pl.BlockSpec((1, send_rows, 128), lambda i: (i, 0, 0)),
            pl.BlockSpec(memory_space=VMEM),
            pl.BlockSpec(memory_space=VMEM),
            pl.BlockSpec(memory_space=VMEM),
        ],
        out_specs=pl.BlockSpec((1, send_rows, 128), lambda i: (i, 0, 0)),
        out_shape=jax.ShapeDtypeStruct((devices, send_rows, 128), jnp.bfloat16),
        cost_estimate=pl.CostEstimate(
            flops=flops, bytes_accessed=4 * devices * rows * 128, transcendentals=flops // 512
        ),
        compiler_params=pltpu.CompilerParams(vmem_limit_bytes=40 << 20),
        name="flash",
    )(q_all, kv_all, all_gates.reshape(devices, 1, rows), gain)
    back = lax.all_to_all(out, "ep", split_axis=0, concat_axis=0, tiled=True)
    if packed:
        back = back.reshape(heads, splits, tile // 2, 2, size).transpose(1, 3, 2, 0, 4)
    else:
        back = back[:, :, size:].reshape(heads, splits, tile, size).transpose(1, 2, 0, 3)
    return back.reshape(rows, width)


def norm_kernel(x_ref, gain_ref, out_ref):
    parts, _, width = x_ref.shape
    pieces = [x_ref[part].astype(jnp.float32) for part in range(parts)]
    square = sum(jnp.sum(p * p, axis=1, keepdims=True) for p in pieces) / (parts * width)
    factor = lax.rsqrt(square + NORM_EPSILON)
    for part, piece in enumerate(pieces):
        lanes = slice(part * width, (part + 1) * width)
        out_ref[:, lanes] = (piece * factor * gain_ref[:, lanes]).astype(out_ref.dtype)


def gated(rows, gate, up):
    dims = (((1,), (1,)), ((), ()))
    gate_value = lax.dot_general(rows, gate, dims, preferred_element_type=jnp.float32)
    up_value = lax.dot_general(rows, up, dims, preferred_element_type=jnp.float32)
    return gate_value / (1.0 + jnp.exp(-gate_value)) * up_value


def hidden_kernel(
    x_ref, routes_ref, weight_ref, gate_ref, up_ref, sgate_ref, sup_ref, hid_ref, shid_ref
):
    expert = pl.program_id(0)
    here = lax.axis_index("ep")
    tokens = shid_ref.shape[0]
    number = here * pl.num_programs(0) + expert
    chunk = min(256, x_ref.shape[0])

    @pl.loop(0, x_ref.shape[0] // chunk)
    def _(step):
        rows = pl.ds(pl.multiple_of(step * chunk, chunk), chunk)
        share = jnp.sum(
            jnp.where(routes_ref[rows, :] == number, weight_ref[rows, :], 0.0),
            axis=1,
            keepdims=True,
        )
        value = gated(x_ref[rows, :], gate_ref[0], up_ref[0])
        hid_ref[0, rows, :] = (value * share).astype(hid_ref.dtype)

    @pl.when(expert == 0)
    def _():
        own = x_ref[pl.ds(pl.multiple_of(here * tokens, tokens), tokens), :]
        shid_ref[...] = gated(own, sgate_ref[...], sup_ref[...]).astype(shid_ref.dtype)


def down_kernel(hid_ref, shid_ref, down_ref, sdown_ref, out_ref):
    tokens = shid_ref.shape[0]
    here = lax.axis_index("ep")
    per_group = down_ref.shape[0]

    @pl.loop(0, hid_ref.shape[1] // tokens)
    def _(step):
        rows = pl.ds(pl.multiple_of(step * tokens, tokens), tokens)
        term = sum(
            jnp.dot(hid_ref[expert, rows, :], down_ref[expert], preferred_element_type=jnp.float32)
            for expert in range(per_group)
        )
        out_ref[0, rows, :] = term.astype(out_ref.dtype)

        @pl.when(step == here)
        def _():
            extra = jnp.dot(shid_ref[...], sdown_ref[...], preferred_element_type=jnp.float32)
            out_ref[0, rows, :] = (term + extra).astype(out_ref.dtype)


def gather_tokens(moe_in):
    slice_width = moe_in.shape[1] // lax.axis_size("tp")
    own_columns = lax.dynamic_slice_in_dim(
        moe_in, lax.axis_index("tp") * slice_width, slice_width, 1
    )
    return lax.all_gather(own_columns, ("ep", "tp"), axis=0)


def expert_terms(
    gathered,
    ffn_gain,
    all_routes,
    all_weights,
    expert_gate,
    expert_up,
    expert_down,
    shared_gate,
    shared_up,
    shared_down,
):
    tokens = gathered.shape[1]
    model_width = ffn_gain.shape[0]
    per_group, hidden_width = expert_gate.shape[:2]
    shared_width = shared_gate.shape[0]
    groups = lax.axis_size("ep")
    parts = lax.axis_size("tp")
    slice_width = model_width // parts
    total = groups * tokens
    params = pltpu.CompilerParams(vmem_limit_bytes=48 << 20)
    whole = pl.BlockSpec(memory_space=VMEM)
    normed = pl.pallas_call(
        norm_kernel,
        grid=(groups,),
        in_specs=[pl.BlockSpec((parts, tokens, slice_width), lambda i: (i, 0, 0)), whole],
        out_specs=pl.BlockSpec((tokens, model_width), lambda i: (i, 0)),
        out_shape=jax.ShapeDtypeStruct((total, model_width), jnp.bfloat16),
        cost_estimate=pl.CostEstimate(
            flops=4 * total * model_width, bytes_accessed=4 * total * model_width, transcendentals=0
        ),
        name="norm",
    )(gathered, ffn_gain[None])
    weight_spec = pl.BlockSpec((1, hidden_width, model_width), lambda i: (i, 0, 0))
    columns = per_group * hidden_width
    hidden, shared_hidden = pl.pallas_call(
        hidden_kernel,
        grid=(per_group,),
        in_specs=[whole, whole, whole, weight_spec, weight_spec, whole, whole],
        out_specs=(
            pl.BlockSpec((1, total, hidden_width), lambda i: (i, 0, 0)),
            pl.BlockSpec((tokens, shared_width), lambda i: (0, 0)),
        ),
        out_shape=(
            jax.ShapeDtypeStruct((per_group, total, hidden_width), jnp.bfloat16),
            jax.ShapeDtypeStruct((tokens, shared_width), jnp.bfloat16),
        ),
        cost_estimate=pl.CostEstimate(
            flops=4 * total * model_width * columns,
            bytes_accessed=4 * columns * model_width,
            transcendentals=total * columns,
        ),
        compiler_params=params,
        name="hidden",
    )(normed, all_routes, all_weights, expert_gate, expert_up, shared_gate, shared_up)
    return pl.pallas_call(
        down_kernel,
        grid=(parts,),
        in_specs=[
            whole,
            whole,
            pl.BlockSpec((per_group, hidden_width, slice_width), lambda i: (0, 0, i)),
            pl.BlockSpec((shared_width, slice_width), lambda i: (0, i)),
        ],
        out_specs=pl.BlockSpec((1, total, slice_width), lambda i: (i, 0, 0)),
        out_shape=jax.ShapeDtypeStruct((parts, total, slice_width), jnp.bfloat16),
        cost_estimate=pl.CostEstimate(
            flops=2 * total * model_width * columns,
            bytes_accessed=2 * (columns + total) * model_width,
            transcendentals=0,
        ),
        compiler_params=params,
        name="down",
    )(hidden, shared_hidden, expert_down, shared_down)


def combine_terms(term):
    groups = lax.axis_size("ep")
    _, total, slice_width = term.shape
    tokens = total // groups
    summed = lax.psum_scatter(term, "tp", scatter_dimension=0, tiled=True)
    back = lax.all_to_all(
        summed.reshape(groups, tokens, slice_width), "ep", split_axis=0, concat_axis=0, tiled=True
    )
    return jnp.sum(back.astype(jnp.float32), axis=0).astype(jnp.bfloat16)


MESH = pl.DeviceIdType.MESH
COPIES = 64
LOG2E = math.log2(math.e)


def flipped(number, mask, bits=3):
    total = 0
    for bit in range(bits):
        digit = lax.rem(number // (1 << bit), 2)
        total = total + ((1 - digit) if (mask >> bit) & 1 else digit) * (1 << bit)
    return total


def fused_kernel(
    cap,
    moe_hbm,
    ffn_hbm,
    routes_hbm,
    weight_hbm,
    cum_hbm,
    k_hbm,
    v_hbm,
    q_hbm,
    gain_hbm,
    egate_hbm,
    eup_hbm,
    edown_hbm,
    sgate_hbm,
    sup_hbm,
    sdown_hbm,
    mixed_ref,
    expert_ref,
    moe_ref,
    ffn_ref,
    routes_ref,
    weight_ref,
    cum_ref,
    k_ref,
    v_ref,
    q_ref,
    gain_ref,
    small_ref,
    kvs,
    qs,
    kv_all,
    q_all,
    kg,
    vt,
    qx,
    small_all,
    peak_buf,
    acc_buf,
    o_send,
    o_recv,
    x_all,
    xg,
    sel_buf,
    share_buf,
    egate,
    eup,
    edown,
    sgate,
    sup,
    sdown,
    y_buf,
    ysh,
    r1,
    r1s,
    s_send,
    ss_send,
    r2,
    r2s,
    term_buf,
    t_send,
    r3,
    u_send,
    r4,
    wsem,
    send_sem,
    recv_sem,
):
    e = lax.axis_index("ep")
    t = lax.axis_index("tp")
    z, x = e // 2, lax.rem(e, 2)
    y, c = t // 2, lax.rem(t, 2)
    ty = (1 - y) * 2 + c
    tc = y * 2 + 1 - c
    rows, width = q_ref.shape
    heads = width // 64
    tile = rows // 2
    half = tile // 2
    tokens, model = moe_ref.shape
    quarter = model // 4
    per_group, hid, _ = egate.shape
    slot2 = 2 * cap
    slots = per_group * slot2

    def peer(m):
        return flipped(e, m)

    def pair(k):
        return flipped(z, k, 2)

    ids = {}

    def remote(name, src, dst, device):
        n = ids.setdefault(name, len(ids))
        return pltpu.make_async_remote_copy(
            src_ref=src,
            dst_ref=dst,
            send_sem=send_sem.at[n],
            recv_sem=recv_sem.at[n],
            device_id=device,
            device_id_type=MESH,
        )

    def block(b, col, count=1):
        return x_all.at[
            pl.ds(pl.multiple_of(b * tokens, tokens), count * tokens),
            pl.ds(pl.multiple_of(col * quarter, quarter), quarter),
        ]

    def small(m):
        return remote(
            ("small", m), small_ref.at[pair(m // 2)], small_all.at[e], {"ep": peer(m)}
        )

    def gz(k):
        b, to = (peer(4), peer(2)) if k == 3 else (e, peer(2 * k))
        return remote(("gz", k), block(b, t), block(b, t), {"ep": to})

    def gx(k):
        b = peer(2 * k)
        return remote(("gx", k), block(b, t), block(b, t), {"ep": peer(1)})

    def pair_rows(k, col):
        if k == 0:
            return block(peer(1), col)
        return block(pair(k) * 2, col, 2)

    def gy(k):
        return remote(("gy", k), pair_rows(k, t), pair_rows(k, t), {"tp": ty})

    def gd0(k):
        return remote(("gd0", k), pair_rows(k, t), pair_rows(k, t), {"tp": tc})

    def gd1(k):
        return remote(("gd1", k), pair_rows(k, ty), pair_rows(k, ty), {"tp": tc})

    def kvz(k):
        return remote(("kvz", k), kvs.at[pair(k)], kv_all.at[e], {"ep": peer(2 * k)})

    def kvx(k):
        b = peer(2 * k)
        return remote(("kvx", k), kv_all.at[b], kv_all.at[b], {"ep": peer(1)})

    def qc(m):
        part = (1 - x) if m % 2 else x
        return remote(("q", m), qs.at[pair(m // 2), part], q_all.at[e], {"ep": peer(m)})

    def c_r1(k):
        return remote(("r1", k), y_buf.at[1 - c, :, k], r1.at[:, k], {"tp": tc})

    def c_r1s():
        return remote("r1s", ysh.at[1 - c], r1s, {"tp": tc})

    def c_r2(k):
        return remote(("r2", k), s_send.at[k], r2.at[k], {"tp": ty})

    def c_r2s():
        return remote("r2s", ss_send, r2s, {"tp": ty})

    def c_r3(k):
        return remote(("r3", k), t_send.at[k], r3.at[k], {"ep": peer(1)})

    def c_r4(k):
        to = peer(2) if k == 3 else peer(2 * k)
        return remote(("r4", k), u_send.at[k], r4.at[k], {"ep": to})

    def c_o(m):
        return remote(("o", m), o_send.at[peer(m)], o_recv.at[e], {"ep": peer(m)})

    started = []

    def start(copy_fn, *args):
        copy_fn(*args).start()
        started.append((copy_fn, args))

    barrier = pltpu.get_barrier_semaphore()
    for m in range(1, 8):
        pl.semaphore_signal(barrier, inc=1, device_id={"ep": peer(m)}, device_id_type=MESH)
    for other in (ty, tc):
        pl.semaphore_signal(barrier, inc=1, device_id={"tp": other}, device_id_type=MESH)

    inputs = (
        (moe_hbm, moe_ref),
        (ffn_hbm, ffn_ref),
        (routes_hbm, routes_ref),
        (weight_hbm, weight_ref),
        (cum_hbm, cum_ref),
        (k_hbm, k_ref),
        (v_hbm, v_ref),
        (q_hbm, q_ref),
        (gain_hbm, gain_ref),
        (sgate_hbm, sgate),
        (sup_hbm, sup),
        (sdown_hbm, sdown),
        (egate_hbm, egate),
        (eup_hbm, eup),
        (edown_hbm, edown),
    )
    loads = [
        pltpu.make_async_copy(src, dst, wsem.at[n]) for n, (src, dst) in enumerate(inputs)
    ]
    for load in loads:
        load.start()

    for load in loads[:2]:
        load.wait()
    own = moe_ref[...].astype(jnp.float32)
    square = jnp.sum(own * own, axis=1, keepdims=True) / model
    own = (own * lax.rsqrt(square + NORM_EPSILON) * ffn_ref[...]).astype(jnp.bfloat16)
    own_rows = pl.ds(pl.multiple_of(e * tokens, tokens), tokens)
    x_all[own_rows, :] = own
    for load in loads[2:5]:
        load.wait()

    lines = rows // 128
    for head in range(heads):
        small_ref[head, 0:4, :] = routes_ref[...].astype(jnp.float32)
        small_ref[head, 4:8, :] = weight_ref[...]
        small_ref[head, 8:16, :] = jnp.concatenate(
            [cum_ref[head : head + 1, r * 128 : (r + 1) * 128] for r in range(lines)]
            + [jnp.zeros((8 - lines, 128), jnp.float32)],
            axis=0,
        )
    small_all[e] = small_ref[z]

    pl.semaphore_wait(barrier, 9)
    for m in (7, 6, 5, 4, 3, 2, 1):
        start(small, m)
    start(gz, 1)
    start(gz, 2)
    start(gx, 0)

    for load in loads[5:9]:
        load.wait()
    low = lax.broadcasted_iota(jnp.int32, (rows, 128), 1) < 64
    low_half = low[:half]
    for head in range(heads):
        lanes = slice(head // 2 * 128, head // 2 * 128 + 128)
        kc, vc = k_ref[:, lanes], v_ref[:, lanes]
        qq = q_ref[:, lanes]
        if head % 2 == 0:
            kvs[head] = jnp.where(low, kc, swap_halves(vc))
        else:
            kvs[head] = jnp.where(low, swap_halves(kc), vc)
        for part in range(2):
            a = qq[part * tile : part * tile + half]
            b = qq[part * tile + half : (part + 1) * tile]
            if head % 2 == 0:
                packed = jnp.where(low_half, a, swap_halves(b))
            else:
                packed = jnp.where(low_half, swap_halves(a), b)
            qs[head, part] = packed
    kv_all[e] = kvs[z]
    q_all[e] = qs[z, x]
    lane = lax.broadcasted_iota(jnp.int32, (1, 128), 1)
    spread = jnp.where(
        lax.broadcasted_iota(jnp.int32, (16, 128), 0) + 64
        == lax.broadcasted_iota(jnp.int32, (16, 128), 1),
        1.0,
        0.0,
    )
    gate_lane = lax.broadcasted_iota(jnp.int32, (16, 128), 0) < 3
    spread = jnp.where(gate_lane, spread, 0.0).astype(jnp.bfloat16)
    pick_value = jnp.where(
        lax.broadcasted_iota(jnp.int32, (64, 128), 0) + 64
        == lax.broadcasted_iota(jnp.int32, (64, 128), 1),
        1.0,
        0.0,
    ).astype(jnp.bfloat16)
    unit = jnp.where(lane < 67, 1.0, 0.0).astype(jnp.bfloat16)
    both = (((1,), (1,)), ((), ()))

    def prep_kv(j):
        kv = kv_all[j]
        left = small_all[j, 8:16, :] * -LOG2E
        split = []
        for _ in range(3):
            piece = left.astype(jnp.bfloat16).astype(jnp.float32)
            split.append(jnp.concatenate([piece[r : r + 1] for r in range(lines)], axis=1))
            left = left - piece
        split.append(jnp.zeros((13, rows), jnp.float32))
        split = jnp.concatenate(split, axis=0).astype(jnp.bfloat16)
        gates = lax.dot_general(
            split, spread, (((0,), (0,)), ((), ())), preferred_element_type=jnp.float32
        )
        kg[j] = jnp.where(low, kv, gates.astype(jnp.bfloat16))
        vt[j] = lax.dot_general(
            pick_value, kv, both, preferred_element_type=jnp.float32
        ).astype(jnp.bfloat16)

    def prep_q(i):
        raw = q_all[i].astype(jnp.float32) * (LOG2E * 64**-0.5)
        first = raw.astype(jnp.bfloat16)
        second = (raw - first.astype(jnp.float32)).astype(jnp.bfloat16)
        zero = jnp.zeros_like(first)
        for n, (value, rest) in enumerate(((first, zero), (second, zero + unit))):
            qx[i, :, n * 128 : (n + 1) * 128] = jnp.concatenate(
                [jnp.where(low_half, value, rest), jnp.where(low_half, swap_halves(value), rest)],
                axis=0,
            )

    def scores_of(j, query):
        keys = jnp.concatenate([kv_all[j], kg[j]], axis=1)
        return lax.dot_general(keys, query, both, preferred_element_type=jnp.float32)

    def update(j, scores, peak, out):
        new_peak = jnp.maximum(peak, jnp.max(scores, axis=0, keepdims=True))
        weights = jnp.exp2(scores - new_peak).astype(jnp.bfloat16)
        out = out * jnp.exp2(peak - new_peak) + jnp.dot(
            vt[j], weights, preferred_element_type=jnp.float32
        )
        return new_peak, out

    def diagonal(k):
        pk = pair(k)
        first, second = qx[2 * pk], qx[2 * pk + 1]
        query = jnp.concatenate([first, second], axis=0)
        scores = scores_of(2 * pk, query)
        later = scores_of(2 * pk + 1, second)
        key_pos = lax.broadcasted_iota(jnp.int32, (rows, 2 * tile), 0)
        row_pos = lax.broadcasted_iota(jnp.int32, (rows, 2 * tile), 1)
        allowed = (key_pos <= row_pos + x * tile) | (row_pos >= tile)
        scores = jnp.where(allowed, scores, -jnp.inf)
        peak = jnp.max(scores, axis=0, keepdims=True)
        weights = jnp.exp2(scores - peak).astype(jnp.bfloat16)
        out = jnp.dot(vt[2 * pk], weights, preferred_element_type=jnp.float32)
        key_pos = lax.broadcasted_iota(jnp.int32, (rows, tile), 0)
        row_pos = lax.broadcasted_iota(jnp.int32, (rows, tile), 1)
        later = jnp.where(key_pos <= row_pos + x * tile, later, -jnp.inf)
        last_peak, last_out = update(2 * pk + 1, later, peak[:, tile:], out[:, tile:])
        peak_buf[pk, :, :tile] = peak[:, :tile]
        peak_buf[pk, :, tile:] = last_peak
        acc_buf[pk, :, :tile] = out[:, :tile]
        acc_buf[pk, :, tile:] = last_out

    def cross(k, m):
        pk, pm = pair(k), pair(m)
        above = (pk - pm + 4) // 4
        hi = pm + above * (pk - pm)
        lo = pk - above * (pk - pm)
        query = jnp.concatenate([qx[2 * hi], qx[2 * hi + 1]], axis=0)
        scores = scores_of(2 * lo, query)
        later = scores_of(2 * lo + 1, query)
        peak, out = update(2 * lo, scores, peak_buf[hi], acc_buf[hi])
        peak, out = update(2 * lo + 1, later, peak, out)
        peak_buf[hi] = peak
        acc_buf[hi] = out

    gain_pair = jnp.where(z // 2 == 0, gain_ref[:, :128], gain_ref[:, 128:])
    gain_swap = swap_halves(gain_pair)
    gain = jnp.where((lane < 64) == (lax.rem(z, 2) == 0), gain_pair, gain_swap)

    def epilogue(k):
        weighted = acc_buf[pair(k)]
        square = jnp.sum(weighted * weighted, axis=0, keepdims=True) / 64
        normed = weighted * lax.rsqrt(square + NORM_EPSILON)
        for xx in range(2):
            at = xx * tile
            out = jnp.concatenate(
                [normed[:, at : at + half], normed[:, at + half : at + tile]], axis=0
            ).T
            o_send[2 * pair(k) + xx] = (out * gain).astype(o_send.dtype)
        for m in (2 * k, 2 * k + 1):
            if m == 0:
                o_recv[e] = o_send[e]
            else:
                start(c_o, m)

    upper = (
        lax.broadcasted_iota(jnp.int32, (tokens, tokens), 0)
        <= lax.broadcasted_iota(jnp.int32, (tokens, tokens), 1)
    )
    upper = jnp.where(upper, 1.0, 0.0).astype(jnp.bfloat16)

    def select(k):
        pk = pair(k)
        named, chosen = [], []
        for bb in range(2):
            table = small_all[2 * pk + bb]
            ids_of = table[0:4].astype(jnp.int32)
            share = table[4:8]
            for j in range(per_group):
                hit = ids_of == e * per_group + j
                named.append(jnp.sum(jnp.where(hit, 1.0, 0.0), axis=0, keepdims=True))
                chosen.append(jnp.sum(jnp.where(hit, share, 0.0), axis=0, keepdims=True))
        flags = jnp.concatenate(named, axis=0)
        rank = jnp.dot(flags.astype(jnp.bfloat16), upper, preferred_element_type=jnp.float32)
        slot = jnp.where(flags > 0.5, rank - 1.0, -1000.0)
        row_of = lax.broadcasted_iota(jnp.int32, (slot2, 2 * tokens), 0).astype(jnp.float32)
        for j in range(per_group):
            target = jnp.concatenate(
                [slot[j : j + 1], slot[per_group + j : per_group + j + 1] + float(cap)], axis=1
            )
            share = jnp.concatenate([chosen[j], chosen[per_group + j]], axis=1)
            match = row_of == target
            sel_buf[k, j * slot2 : (j + 1) * slot2, :] = jnp.where(match, 1.0, 0.0).astype(
                jnp.bfloat16
            )
            share_buf[j, k * slot2 : (k + 1) * slot2, :] = jnp.sum(
                jnp.where(match, share, 0.0), axis=1, keepdims=True
            )

    def pick(k):
        gd0(k).wait_recv()
        gd1(k).wait_recv()
        pair_at = pl.ds(pl.multiple_of(pair(k) * 2 * tokens, 2 * tokens), 2 * tokens)
        for part in range(4):
            cols = slice(part * quarter, (part + 1) * quarter)
            picked = jnp.dot(
                sel_buf[k], x_all[pair_at, cols], preferred_element_type=jnp.float32
            ).astype(jnp.bfloat16)
            for j in range(per_group):
                xg[j, k * slot2 : (k + 1) * slot2, cols] = picked[j * slot2 : (j + 1) * slot2]

    def e1(k):
        gz(k).wait_recv()
        start(gx, k)

    def e2(k):
        gx(k).wait_recv()
        start(gy, k)
        start(gd0, k)

    def e3(k):
        gy(k).wait_recv()
        start(gd1, k)

    def forward(k):
        kvz(k).wait_recv()
        start(kvx, k)

    def ready(k):
        kvx(k).wait_recv()
        for m in (2 * k, 2 * k + 1):
            if m:
                qc(m).wait_recv()
            prep_kv(peer(m))
            prep_q(peer(m))

    for load in loads[9:12]:
        load.wait()
    shared_hidden = gated(x_all[own_rows, :], sgate[...], sup[...]).astype(jnp.bfloat16)
    for part in range(4):
        cols = slice(part * quarter, (part + 1) * quarter)
        ysh[part % 2, part // 2] = jnp.dot(
            shared_hidden, sdown[:, cols], preferred_element_type=jnp.float32
        ).astype(jnp.bfloat16)
    def experts_of(chunk):
        span = 2 * slot2

        @pl.loop(0, per_group, unroll=2)
        def _(j):
            here = slice(chunk * span, (chunk + 1) * span)
            value = gated(xg[j, here, :], egate[j], eup[j])
            hidden = (value * share_buf[j, here, :]).astype(jnp.bfloat16)
            at = pl.ds(pl.multiple_of(j * slot2, 16), slot2)
            for part in range(4):
                cols = slice(part * quarter, (part + 1) * quarter)
                out = jnp.dot(
                    hidden, edown[j, :, cols], preferred_element_type=jnp.float32
                ).astype(jnp.bfloat16)
                for k in range(2):
                    y_buf[part % 2, part // 2, 2 * chunk + k, at, :] = out[
                        k * slot2 : (k + 1) * slot2
                    ]

    def wide(ref):
        return ref.astype(jnp.float32)

    def core_sum(k):
        c_r1(k).wait_recv()
        s_send[k] = (wide(y_buf[c, 1 - y, k]) + wide(r1[1 - y, k])).astype(jnp.bfloat16)
        c_r2(k).start()

    def shared_sum():
        c_r1s().wait_recv()
        ss_send[...] = (wide(ysh[c, 1 - y]) + wide(r1s[1 - y])).astype(jnp.bfloat16)
        c_r2s().start()

    def scatter(k):
        c_r2(k).wait_recv()
        total = wide(y_buf[c, y, k]) + wide(r1[y, k]) + wide(r2[k])
        term = lax.dot_general(
            sel_buf[k],
            total.astype(jnp.bfloat16),
            (((0,), (0,)), ((), ())),
            preferred_element_type=jnp.float32,
        )
        term_buf[k, 0] = term[:tokens]
        term_buf[k, 1] = term[tokens:]
        t_send[k] = term_buf[k, 1 - x].astype(jnp.bfloat16)
        c_r3(k).start()

    def combine(k):
        c_r3(k).wait_recv()
        total = term_buf[k, x] + wide(r3[k])
        if k == 2:
            c_r4(3).wait_recv()
            total = total + wide(r4[3])
        u_send[k] = total.astype(jnp.bfloat16)
        c_r4(k).start()

    for k in range(4):
        started.append((c_r2, (k,)))
        started.append((c_r3, (k,)))
        if k:
            started.append((c_r4, (k,)))
    started.append((c_r2s, ()))

    start(c_r1s)
    for m in range(1, 8):
        small(m).wait_recv()
    for k in range(4):
        select(k)
    shared_sum()
    e2(0)
    e1(2)
    start(gz, 3)
    e1(1)
    for k in (3, 2, 1):
        start(kvz, k)
        start(qc, 2 * k)
    e3(0)
    e2(2)
    pick(0)
    e1(3)
    start(kvx, 0)
    for m in (1, 7, 5, 3):
        start(qc, m)
    e2(3)
    e2(1)
    e3(2)
    pick(2)
    ready(0)
    diagonal(0)
    forward(3)
    e3(3)
    for load in loads[12:]:
        load.wait()
    pick(3)
    experts_of(1)
    e3(1)
    start(c_r1, 3)
    start(c_r1, 2)
    ready(3)
    diagonal(3)
    core_sum(3)
    core_sum(2)
    pick(1)
    forward(2)
    experts_of(0)
    start(c_r1, 1)
    start(c_r1, 0)
    forward(1)
    ready(2)
    scatter(3)
    core_sum(1)
    core_sum(0)
    diagonal(2)
    cross(3, 0)
    scatter(2)
    cross(2, 0)
    combine(3)
    cross(2, 3)
    scatter(1)
    ready(1)
    diagonal(1)
    combine(2)
    scatter(0)
    cross(1, 3)
    epilogue(3)
    combine(1)
    cross(1, 2)
    epilogue(2)
    cross(1, 0)
    epilogue(1)
    epilogue(0)
    c_r2s().wait_recv()
    c_r3(0).wait_recv()
    out = term_buf[0, x] + wide(r3[0]) + wide(ysh[c, y]) + wide(r1s[y]) + wide(r2s[...])
    for k in (2, 1):
        c_r4(k).wait_recv()
        out = out + wide(r4[k])
    expert_ref[...] = out.astype(expert_ref.dtype)

    for m in range(1, 8):
        c_o(m).wait_recv()
    mixed_ref[...] = o_recv[...]
    for copy_fn, args in started:
        copy_fn(*args).wait_send()


def finish_kernel(parcels_ref, sum_ref, mixed_ref, expert_ref):
    count, half, _ = parcels_ref.shape
    low_half = lax.broadcasted_iota(jnp.int32, (half, 128), 1) < 64
    for part in range(2):
        for head in range(0, count // 2, 2):
            lanes = slice(head // 2 * 128, head // 2 * 128 + 128)
            first, second = parcels_ref[head * 2 + part], parcels_ref[(head + 1) * 2 + part]
            at = part * 2 * half
            mixed_ref[at : at + half, lanes] = jnp.where(low_half, first, swap_halves(second))
            mixed_ref[at + half : at + 2 * half, lanes] = jnp.where(
                low_half, swap_halves(first), second
            )
    expert_ref[...] = sum_ref[...]


def fused(
    queries,
    keys,
    values,
    cum_gate,
    head_gain,
    moe_in,
    ffn_gain,
    routes,
    route_weight,
    expert_gate,
    expert_up,
    expert_down,
    shared_gate,
    shared_up,
    shared_down,
):
    rows, heads = cum_gate.shape
    width = queries.shape[1]
    tokens, model = moe_in.shape
    choose = routes.shape[1]
    per_group, hid, _ = expert_gate.shape
    experts = per_group * lax.axis_size("ep")
    cap = 3 * tokens * choose // (2 * experts)
    devices = lax.axis_size("ep")
    tile, half, quarter = rows // 2, rows // 4, model // 4
    slots = per_group * 2 * cap
    shared = shared_gate.shape[0]
    bf16, f32 = jnp.bfloat16, jnp.float32
    vmem = pl.BlockSpec(memory_space=VMEM)
    hbm = pl.BlockSpec(memory_space=pl.ANY)
    scratch = [
        VMEM((tokens, model), bf16),
        VMEM((1, model), f32),
        VMEM((choose, tokens), jnp.int32),
        VMEM((choose, tokens), f32),
        VMEM((heads, rows), f32),
        VMEM((rows, width), bf16),
        VMEM((rows, width), bf16),
        VMEM((rows, width), bf16),
        VMEM((1, width), f32),
        VMEM((heads, 16, 128), f32),
        VMEM((heads, rows, 128), bf16),
        VMEM((heads, 2, half, 128), bf16),
        VMEM((devices, rows, 128), bf16),
        VMEM((devices, half, 128), bf16),
        VMEM((devices, rows, 128), bf16),
        VMEM((devices, 64, rows), bf16),
        VMEM((devices, tile, 256), bf16),
        VMEM((devices, 16, 128), f32),
        VMEM((4, 1, 2 * tile), f32),
        VMEM((4, 64, 2 * tile), f32),
        VMEM((devices, half, 128), bf16),
        VMEM((devices, half, 128), bf16),
        VMEM((devices * tokens, model), bf16),
        VMEM((per_group, 8 * cap, model), bf16),
        VMEM((4, slots, 2 * tokens), bf16),
        VMEM((per_group, 8 * cap, 1), f32),
        VMEM((per_group, hid, model), bf16),
        VMEM((per_group, hid, model), bf16),
        VMEM((per_group, hid, model), bf16),
        VMEM((shared, model), bf16),
        VMEM((shared, model), bf16),
        VMEM((shared, model), bf16),
        VMEM((2, 2, 4, slots, quarter), bf16),
        VMEM((2, 2, tokens, quarter), bf16),
        VMEM((2, 4, slots, quarter), bf16),
        VMEM((2, tokens, quarter), bf16),
        VMEM((4, slots, quarter), bf16),
        VMEM((tokens, quarter), bf16),
        VMEM((4, slots, quarter), bf16),
        VMEM((tokens, quarter), bf16),
        VMEM((4, 2, tokens, quarter), f32),
        VMEM((4, tokens, quarter), bf16),
        VMEM((4, tokens, quarter), bf16),
        VMEM((4, tokens, quarter), bf16),
        VMEM((4, tokens, quarter), bf16),
        pltpu.SemaphoreType.DMA((15,)),
        pltpu.SemaphoreType.DMA((COPIES,)),
        pltpu.SemaphoreType.DMA((COPIES,)),
    ]
    parcels, total = pl.pallas_call(
        functools.partial(fused_kernel, cap),
        in_specs=[hbm] * 15,
        out_specs=(vmem, vmem),
        out_shape=(
            jax.ShapeDtypeStruct((devices, half, 128), bf16),
            jax.ShapeDtypeStruct((tokens, quarter), bf16),
        ),
        scratch_shapes=scratch,
        compiler_params=pltpu.CompilerParams(
            collective_id=0, has_side_effects=True, vmem_limit_bytes=62 << 20
        ),
        name="fused",
    )(
        moe_in,
        ffn_gain[None],
        routes.T,
        route_weight.T,
        cum_gate.T,
        keys,
        values,
        queries,
        head_gain[None],
        expert_gate,
        expert_up,
        expert_down,
        shared_gate,
        shared_up,
        shared_down,
    )
    return pl.pallas_call(
        finish_kernel,
        in_specs=[vmem, vmem],
        out_specs=(vmem, vmem),
        out_shape=(
            jax.ShapeDtypeStruct((rows, width), bf16),
            jax.ShapeDtypeStruct((tokens, quarter), bf16),
        ),
        name="finish",
    )(parcels, total)


def fits_fused(cum_gate, queries, moe_in, routes, expert_gate):
    rows, heads = cum_gate.shape
    tokens, choose = routes.shape
    per_group = expert_gate.shape[0]
    devices = lax.axis_size("ep")
    cap = 3 * tokens * choose // (2 * per_group * devices)
    return (
        devices == 8
        and lax.axis_size("tp") == 4
        and heads == 4
        and queries.shape[1] == 256
        and rows % 128 == 0
        and rows // 128 <= 8
        and (rows // 4) % 16 == 0
        and tokens == 128
        and choose == 4
        and per_group == 4
        and (2 * cap) % 16 == 0
    )


def on_device(
    queries,
    keys,
    values,
    cum_gate,
    head_gain,
    moe_in,
    ffn_gain,
    routes,
    route_weight,
    expert_gate,
    expert_up,
    expert_down,
    shared_gate,
    shared_up,
    shared_down,
):
    if fits_fused(cum_gate, queries, moe_in, routes, expert_gate):
        return fused(
            queries,
            keys,
            values,
            cum_gate,
            head_gain,
            moe_in,
            ffn_gain,
            routes,
            route_weight,
            expert_gate,
            expert_up,
            expert_down,
            shared_gate,
            shared_up,
            shared_down,
        )
    rows, heads = cum_gate.shape
    gathered = gather_tokens(moe_in)
    got, packed = trade_rows(queries, keys, values, heads)
    all_gates, all_routes, all_weights = trade_small(cum_gate, routes, route_weight)
    gathered, got = lax.optimization_barrier((gathered, got))
    term = expert_terms(
        gathered,
        ffn_gain,
        all_routes,
        all_weights,
        expert_gate,
        expert_up,
        expert_down,
        shared_gate,
        shared_up,
        shared_down,
    )
    term, got = lax.optimization_barrier((term, got))
    mixed = attend(got, packed, rows, all_gates, heads, head_gain)
    return (mixed, combine_terms(term))


def solution(mesh):
    in_specs = (
        P("ep", "tp"),
        P("ep", "tp"),
        P("ep", "tp"),
        P("ep", "tp"),
        P("tp"),
        P("ep", None),
        P(),
        P("ep", None),
        P("ep", None),
        P("ep", "tp", None),
        P("ep", "tp", None),
        P("ep", "tp", None),
        P("tp", None),
        P("tp", None),
        P("tp", None),
    )
    out_specs = (P("ep", "tp"), P("ep", "tp"))
    return jax.shard_map(
        on_device, mesh=mesh, in_specs=in_specs, out_specs=out_specs, check_vma=False
    )
```

```python
import functools
import math

import jax
import jax.numpy as jnp
from jax import lax
from jax.experimental import pallas as pl
from jax.experimental.pallas import tpu as pltpu
from jax.sharding import PartitionSpec as P

NORM_EPSILON = 1e-06
VMEM = pltpu.VMEM


def swap_halves(x):
    half = x.shape[1] // 2
    return jnp.concatenate([x[:, half:], x[:, :half]], axis=1)


def pack_kernel(splits, scale, q_ref, k_ref, v_ref, kv_ref, qp_ref):
    rows, width = q_ref.shape
    tile = rows // splits
    half = tile // 2
    low = lax.broadcasted_iota(jnp.int32, (rows, 128), 1) < 64
    low_half = low[:half]
    for head in range(width // 64):
        lanes = slice(head // 2 * 128, head // 2 * 128 + 128)
        kc, vc = k_ref[:, lanes], v_ref[:, lanes]
        qc = q_ref[:, lanes] * jnp.asarray(scale, q_ref.dtype)
        if head % 2 == 0:
            kv_ref[head] = jnp.where(low, kc, swap_halves(vc))
        else:
            kv_ref[head] = jnp.where(low, swap_halves(kc), vc)
        for part in range(splits):
            a = qc[part * tile : part * tile + half]
            b = qc[part * tile + half : (part + 1) * tile]
            if head % 2 == 0:
                packed = jnp.where(low_half, a, swap_halves(b))
            else:
                packed = jnp.where(low_half, swap_halves(a), b)
            qp_ref[head * splits + part] = packed


def flash_kernel(splits, packed, key_len, q_ref, kv_ref, gate_ref, gain_ref, out_ref):
    block = pl.program_id(0)
    part = lax.rem(lax.axis_index("ep"), splits)
    raw = q_ref[0]
    half = raw.shape[0]
    if packed:
        low = lax.broadcasted_iota(jnp.int32, raw.shape, 1) < 64
        zero = jnp.zeros_like(raw)
        query = jnp.concatenate(
            [jnp.where(low, raw, zero), jnp.where(low, swap_halves(raw), zero)], axis=0
        )
    else:
        query = raw
    rows = query.shape[0]

    def visit(step, state, masked):
        peak, weighted = state
        keys = kv_ref[pl.ds(pl.multiple_of(step * key_len, key_len), key_len), :]
        scores = lax.dot_general(
            query, keys, (((1,), (1,)), ((), ())), preferred_element_type=jnp.float32
        )
        scores = scores - gate_ref[step]
        if masked:
            row_pos = part * rows + lax.broadcasted_iota(jnp.int32, scores.shape, 0)
            key_pos = lax.broadcasted_iota(jnp.int32, scores.shape, 1)
            scores = jnp.where(key_pos <= row_pos, scores, -jnp.inf)
        new_peak = jnp.maximum(peak, jnp.max(scores, axis=1, keepdims=True))
        weights = jnp.exp(scores - new_peak).astype(jnp.bfloat16)
        weighted = weighted * jnp.exp(peak - new_peak) + jnp.dot(
            weights, keys, preferred_element_type=jnp.float32
        )
        return new_peak, weighted

    state = (jnp.full((rows, 1), -1e30, jnp.float32), jnp.zeros((rows, 128), jnp.float32))
    state = visit(block, state, True)
    state = lax.fori_loop(0, block, lambda step, s: visit(step, s, False), state)
    _, weighted = state
    high = lax.broadcasted_iota(jnp.int32, weighted.shape, 1) >= 64
    square = jnp.sum(jnp.where(high, weighted * weighted, 0.0), axis=1, keepdims=True) / 64
    normed = weighted * lax.rsqrt(square + NORM_EPSILON) * gain_ref[...]
    if packed:
        normed = jnp.where(high[:half], normed[half:], swap_halves(normed[:half]))
    out_ref[0] = normed.astype(out_ref.dtype)


def trade_small(cum_gate, routes, route_weight):
    rows, heads = cum_gate.shape
    devices = lax.axis_size("ep")
    tokens, choose = routes.shape
    gates = jnp.repeat(cum_gate.T, devices // heads, axis=0)
    named = jnp.concatenate([routes.astype(jnp.float32).reshape(-1), route_weight.reshape(-1)])
    small = jnp.concatenate([gates, jnp.broadcast_to(named, (devices, named.size))], axis=1)
    small = lax.all_to_all(small, "ep", split_axis=0, concat_axis=0, tiled=True)
    count = tokens * choose
    all_routes = small[:, rows : rows + count].astype(jnp.int32).reshape(-1, choose)
    all_weights = small[:, rows + count :].reshape(-1, choose)
    return small[:, :rows], all_routes, all_weights


def trade_rows(queries, keys, values, heads):
    rows, width = queries.shape
    size = width // heads
    devices = lax.axis_size("ep")
    splits = devices // heads
    tile = rows // splits
    scale = size**-0.5
    packed = heads % 2 == 0 and (tile // 2) % 16 == 0
    send_rows = tile // 2 if packed else tile
    if packed:
        kv, qp = pl.pallas_call(
            functools.partial(pack_kernel, splits, scale),
            out_shape=(
                jax.ShapeDtypeStruct((heads, rows, 128), jnp.bfloat16),
                jax.ShapeDtypeStruct((devices, send_rows, 128), jnp.bfloat16),
            ),
            name="pack",
        )(queries, keys, values)
    else:
        kv = jnp.concatenate(
            [keys.reshape(rows, heads, size), values.reshape(rows, heads, size)], axis=2
        ).transpose(1, 0, 2)
        qs = (queries * jnp.asarray(scale, queries.dtype)).reshape(splits, tile, heads, size)
        qs = qs.transpose(2, 0, 1, 3).reshape(devices, tile, size)
        qp = jnp.concatenate([qs, jnp.zeros_like(qs)], axis=2)
    parcel = jnp.concatenate([jnp.repeat(kv, splits, axis=0), qp], axis=1)
    return lax.all_to_all(parcel, "ep", split_axis=0, concat_axis=0, tiled=True), packed


def attend(got, packed, rows, all_gates, heads, head_gain):
    devices, parcel_rows, _ = got.shape
    width = head_gain.shape[0]
    size = width // heads
    splits = devices // heads
    tile = rows // splits
    send_rows = parcel_rows - rows
    kv_all = got[:, :rows].reshape(devices * rows, 128)
    q_all = got[:, rows:]
    head = lax.axis_index("ep") // splits
    gain = lax.dynamic_slice_in_dim(head_gain, head * size, size, 0)
    gain = jnp.concatenate([gain, gain])[None]
    flops = 2 * 2 * 128 * devices * (devices + 1) // 2 * tile * rows
    out = pl.pallas_call(
        functools.partial(flash_kernel, splits, packed, rows),
        grid=(devices,),
        in_specs=[
            pl.BlockSpec((1, send_rows, 128), lambda i: (i, 0, 0)),
            pl.BlockSpec(memory_space=VMEM),
            pl.BlockSpec(memory_space=VMEM),
            pl.BlockSpec(memory_space=VMEM),
        ],
        out_specs=pl.BlockSpec((1, send_rows, 128), lambda i: (i, 0, 0)),
        out_shape=jax.ShapeDtypeStruct((devices, send_rows, 128), jnp.bfloat16),
        cost_estimate=pl.CostEstimate(
            flops=flops, bytes_accessed=4 * devices * rows * 128, transcendentals=flops // 512
        ),
        compiler_params=pltpu.CompilerParams(vmem_limit_bytes=40 << 20),
        name="flash",
    )(q_all, kv_all, all_gates.reshape(devices, 1, rows), gain)
    back = lax.all_to_all(out, "ep", split_axis=0, concat_axis=0, tiled=True)
    if packed:
        back = back.reshape(heads, splits, tile // 2, 2, size).transpose(1, 3, 2, 0, 4)
    else:
        back = back[:, :, size:].reshape(heads, splits, tile, size).transpose(1, 2, 0, 3)
    return back.reshape(rows, width)


def norm_kernel(x_ref, gain_ref, out_ref):
    parts, _, width = x_ref.shape
    pieces = [x_ref[part].astype(jnp.float32) for part in range(parts)]
    square = sum(jnp.sum(p * p, axis=1, keepdims=True) for p in pieces) / (parts * width)
    factor = lax.rsqrt(square + NORM_EPSILON)
    for part, piece in enumerate(pieces):
        lanes = slice(part * width, (part + 1) * width)
        out_ref[:, lanes] = (piece * factor * gain_ref[:, lanes]).astype(out_ref.dtype)


def gated(rows, gate, up):
    dims = (((1,), (1,)), ((), ()))
    gate_value = lax.dot_general(rows, gate, dims, preferred_element_type=jnp.float32)
    up_value = lax.dot_general(rows, up, dims, preferred_element_type=jnp.float32)
    return gate_value / (1.0 + jnp.exp(-gate_value)) * up_value


def hidden_kernel(
    x_ref, routes_ref, weight_ref, gate_ref, up_ref, sgate_ref, sup_ref, hid_ref, shid_ref
):
    expert = pl.program_id(0)
    here = lax.axis_index("ep")
    tokens = shid_ref.shape[0]
    number = here * pl.num_programs(0) + expert
    chunk = min(256, x_ref.shape[0])

    @pl.loop(0, x_ref.shape[0] // chunk)
    def _(step):
        rows = pl.ds(pl.multiple_of(step * chunk, chunk), chunk)
        share = jnp.sum(
            jnp.where(routes_ref[rows, :] == number, weight_ref[rows, :], 0.0),
            axis=1,
            keepdims=True,
        )
        value = gated(x_ref[rows, :], gate_ref[0], up_ref[0])
        hid_ref[0, rows, :] = (value * share).astype(hid_ref.dtype)

    @pl.when(expert == 0)
    def _():
        own = x_ref[pl.ds(pl.multiple_of(here * tokens, tokens), tokens), :]
        shid_ref[...] = gated(own, sgate_ref[...], sup_ref[...]).astype(shid_ref.dtype)


def down_kernel(hid_ref, shid_ref, down_ref, sdown_ref, out_ref):
    tokens = shid_ref.shape[0]
    here = lax.axis_index("ep")
    per_group = down_ref.shape[0]

    @pl.loop(0, hid_ref.shape[1] // tokens)
    def _(step):
        rows = pl.ds(pl.multiple_of(step * tokens, tokens), tokens)
        term = sum(
            jnp.dot(hid_ref[expert, rows, :], down_ref[expert], preferred_element_type=jnp.float32)
            for expert in range(per_group)
        )
        out_ref[0, rows, :] = term.astype(out_ref.dtype)

        @pl.when(step == here)
        def _():
            extra = jnp.dot(shid_ref[...], sdown_ref[...], preferred_element_type=jnp.float32)
            out_ref[0, rows, :] = (term + extra).astype(out_ref.dtype)


def gather_tokens(moe_in):
    slice_width = moe_in.shape[1] // lax.axis_size("tp")
    own_columns = lax.dynamic_slice_in_dim(
        moe_in, lax.axis_index("tp") * slice_width, slice_width, 1
    )
    return lax.all_gather(own_columns, ("ep", "tp"), axis=0)


def expert_terms(
    gathered,
    ffn_gain,
    all_routes,
    all_weights,
    expert_gate,
    expert_up,
    expert_down,
    shared_gate,
    shared_up,
    shared_down,
):
    tokens = gathered.shape[1]
    model_width = ffn_gain.shape[0]
    per_group, hidden_width = expert_gate.shape[:2]
    shared_width = shared_gate.shape[0]
    groups = lax.axis_size("ep")
    parts = lax.axis_size("tp")
    slice_width = model_width // parts
    total = groups * tokens
    params = pltpu.CompilerParams(vmem_limit_bytes=48 << 20)
    whole = pl.BlockSpec(memory_space=VMEM)
    normed = pl.pallas_call(
        norm_kernel,
        grid=(groups,),
        in_specs=[pl.BlockSpec((parts, tokens, slice_width), lambda i: (i, 0, 0)), whole],
        out_specs=pl.BlockSpec((tokens, model_width), lambda i: (i, 0)),
        out_shape=jax.ShapeDtypeStruct((total, model_width), jnp.bfloat16),
        cost_estimate=pl.CostEstimate(
            flops=4 * total * model_width, bytes_accessed=4 * total * model_width, transcendentals=0
        ),
        name="norm",
    )(gathered, ffn_gain[None])
    weight_spec = pl.BlockSpec((1, hidden_width, model_width), lambda i: (i, 0, 0))
    columns = per_group * hidden_width
    hidden, shared_hidden = pl.pallas_call(
        hidden_kernel,
        grid=(per_group,),
        in_specs=[whole, whole, whole, weight_spec, weight_spec, whole, whole],
        out_specs=(
            pl.BlockSpec((1, total, hidden_width), lambda i: (i, 0, 0)),
            pl.BlockSpec((tokens, shared_width), lambda i: (0, 0)),
        ),
        out_shape=(
            jax.ShapeDtypeStruct((per_group, total, hidden_width), jnp.bfloat16),
            jax.ShapeDtypeStruct((tokens, shared_width), jnp.bfloat16),
        ),
        cost_estimate=pl.CostEstimate(
            flops=4 * total * model_width * columns,
            bytes_accessed=4 * columns * model_width,
            transcendentals=total * columns,
        ),
        compiler_params=params,
        name="hidden",
    )(normed, all_routes, all_weights, expert_gate, expert_up, shared_gate, shared_up)
    return pl.pallas_call(
        down_kernel,
        grid=(parts,),
        in_specs=[
            whole,
            whole,
            pl.BlockSpec((per_group, hidden_width, slice_width), lambda i: (0, 0, i)),
            pl.BlockSpec((shared_width, slice_width), lambda i: (0, i)),
        ],
        out_specs=pl.BlockSpec((1, total, slice_width), lambda i: (i, 0, 0)),
        out_shape=jax.ShapeDtypeStruct((parts, total, slice_width), jnp.bfloat16),
        cost_estimate=pl.CostEstimate(
            flops=2 * total * model_width * columns,
            bytes_accessed=2 * (columns + total) * model_width,
            transcendentals=0,
        ),
        compiler_params=params,
        name="down",
    )(hidden, shared_hidden, expert_down, shared_down)


def combine_terms(term):
    groups = lax.axis_size("ep")
    _, total, slice_width = term.shape
    tokens = total // groups
    summed = lax.psum_scatter(term, "tp", scatter_dimension=0, tiled=True)
    back = lax.all_to_all(
        summed.reshape(groups, tokens, slice_width), "ep", split_axis=0, concat_axis=0, tiled=True
    )
    return jnp.sum(back.astype(jnp.float32), axis=0).astype(jnp.bfloat16)


MESH = pl.DeviceIdType.MESH
COPIES = 64
LOG2E = math.log2(math.e)


def flipped(number, mask, bits=3):
    total = 0
    for bit in range(bits):
        digit = lax.rem(number // (1 << bit), 2)
        total = total + ((1 - digit) if (mask >> bit) & 1 else digit) * (1 << bit)
    return total


def fused_kernel(
    cap,
    moe_hbm,
    ffn_hbm,
    routes_hbm,
    weight_hbm,
    cum_hbm,
    k_hbm,
    v_hbm,
    q_hbm,
    gain_hbm,
    egate_hbm,
    eup_hbm,
    edown_hbm,
    sgate_hbm,
    sup_hbm,
    sdown_hbm,
    mixed_ref,
    expert_ref,
    moe_ref,
    ffn_ref,
    routes_ref,
    weight_ref,
    cum_ref,
    k_ref,
    v_ref,
    q_ref,
    gain_ref,
    small_ref,
    kvs,
    qs,
    kv_all,
    q_all,
    kg,
    vt,
    qx,
    small_all,
    peak_buf,
    acc_buf,
    o_send,
    o_recv,
    x_all,
    xg,
    sel_buf,
    share_buf,
    egate,
    eup,
    edown,
    sgate,
    sup,
    sdown,
    y_buf,
    ysh,
    r1,
    r1s,
    s_send,
    ss_send,
    r2,
    r2s,
    term_buf,
    t_send,
    r3,
    u_send,
    r4,
    wsem,
    send_sem,
    recv_sem,
):
    e = lax.axis_index("ep")
    t = lax.axis_index("tp")
    z, x = e // 2, lax.rem(e, 2)
    y, c = t // 2, lax.rem(t, 2)
    ty = (1 - y) * 2 + c
    tc = y * 2 + 1 - c
    rows, width = q_ref.shape
    heads = width // 64
    tile = rows // 2
    half = tile // 2
    tokens, model = moe_ref.shape
    quarter = model // 4
    per_group, hid, _ = egate.shape
    slot2 = 2 * cap
    slots = per_group * slot2

    def peer(m):
        return flipped(e, m)

    def pair(k):
        return flipped(z, k, 2)

    ids = {}

    def remote(name, src, dst, device):
        n = ids.setdefault(name, len(ids))
        return pltpu.make_async_remote_copy(
            src_ref=src,
            dst_ref=dst,
            send_sem=send_sem.at[n],
            recv_sem=recv_sem.at[n],
            device_id=device,
            device_id_type=MESH,
        )

    def block(b, col, count=1):
        return x_all.at[
            pl.ds(pl.multiple_of(b * tokens, tokens), count * tokens),
            pl.ds(pl.multiple_of(col * quarter, quarter), quarter),
        ]

    def small(m):
        return remote(
            ("small", m), small_ref.at[pair(m // 2)], small_all.at[e], {"ep": peer(m)}
        )

    def gz(k):
        b, to = (peer(4), peer(2)) if k == 3 else (e, peer(2 * k))
        return remote(("gz", k), block(b, t), block(b, t), {"ep": to})

    def gx(k):
        b = peer(2 * k)
        return remote(("gx", k), block(b, t), block(b, t), {"ep": peer(1)})

    def pair_rows(k, col):
        if k == 0:
            return block(peer(1), col)
        return block(pair(k) * 2, col, 2)

    def gy(k):
        return remote(("gy", k), pair_rows(k, t), pair_rows(k, t), {"tp": ty})

    def gd0(k):
        return remote(("gd0", k), pair_rows(k, t), pair_rows(k, t), {"tp": tc})

    def gd1(k):
        return remote(("gd1", k), pair_rows(k, ty), pair_rows(k, ty), {"tp": tc})

    def kvz(k):
        return remote(("kvz", k), kvs.at[pair(k)], kv_all.at[e], {"ep": peer(2 * k)})

    def kvx(k):
        b = peer(2 * k)
        return remote(("kvx", k), kv_all.at[b], kv_all.at[b], {"ep": peer(1)})

    def qc(m):
        part = (1 - x) if m % 2 else x
        return remote(("q", m), qs.at[pair(m // 2), part], q_all.at[e], {"ep": peer(m)})

    def c_r1(k):
        return remote(("r1", k), y_buf.at[1 - c, :, k], r1.at[:, k], {"tp": tc})

    def c_r1s():
        return remote("r1s", ysh.at[1 - c], r1s, {"tp": tc})

    def c_r2(k):
        return remote(("r2", k), s_send.at[k], r2.at[k], {"tp": ty})

    def c_r2s():
        return remote("r2s", ss_send, r2s, {"tp": ty})

    def c_r3(k):
        return remote(("r3", k), t_send.at[k], r3.at[k], {"ep": peer(1)})

    def c_r4(k):
        to = peer(2) if k == 3 else peer(2 * k)
        return remote(("r4", k), u_send.at[k], r4.at[k], {"ep": to})

    def c_o(m):
        return remote(("o", m), o_send.at[peer(m)], o_recv.at[e], {"ep": peer(m)})

    started = []

    def start(copy_fn, *args):
        copy_fn(*args).start()
        started.append((copy_fn, args))

    barrier = pltpu.get_barrier_semaphore()
    for m in range(1, 8):
        pl.semaphore_signal(barrier, inc=1, device_id={"ep": peer(m)}, device_id_type=MESH)
    for other in (ty, tc):
        pl.semaphore_signal(barrier, inc=1, device_id={"tp": other}, device_id_type=MESH)

    inputs = (
        (moe_hbm, moe_ref),
        (ffn_hbm, ffn_ref),
        (routes_hbm, routes_ref),
        (weight_hbm, weight_ref),
        (cum_hbm, cum_ref),
        (k_hbm, k_ref),
        (v_hbm, v_ref),
        (q_hbm, q_ref),
        (gain_hbm, gain_ref),
        (sgate_hbm, sgate),
        (sup_hbm, sup),
        (sdown_hbm, sdown),
        (egate_hbm, egate),
        (eup_hbm, eup),
        (edown_hbm, edown),
    )
    loads = [
        pltpu.make_async_copy(src, dst, wsem.at[n]) for n, (src, dst) in enumerate(inputs)
    ]
    for load in loads:
        load.start()

    for load in loads[:2]:
        load.wait()
    own = moe_ref[...].astype(jnp.float32)
    square = jnp.sum(own * own, axis=1, keepdims=True) / model
    own = (own * lax.rsqrt(square + NORM_EPSILON) * ffn_ref[...]).astype(jnp.bfloat16)
    own_rows = pl.ds(pl.multiple_of(e * tokens, tokens), tokens)
    x_all[own_rows, :] = own
    for load in loads[2:5]:
        load.wait()

    lines = rows // 128
    for head in range(heads):
        small_ref[head, 0:4, :] = routes_ref[...].astype(jnp.float32)
        small_ref[head, 4:8, :] = weight_ref[...]
        small_ref[head, 8:16, :] = jnp.concatenate(
            [cum_ref[head : head + 1, r * 128 : (r + 1) * 128] for r in range(lines)]
            + [jnp.zeros((8 - lines, 128), jnp.float32)],
            axis=0,
        )
    small_all[e] = small_ref[z]

    pl.semaphore_wait(barrier, 9)
    for m in (7, 6, 5, 4, 3, 2, 1):
        start(small, m)
    start(gz, 1)
    start(gz, 2)
    start(gx, 0)

    for load in loads[5:9]:
        load.wait()
    low = lax.broadcasted_iota(jnp.int32, (rows, 128), 1) < 64
    low_half = low[:half]
    for head in range(heads):
        lanes = slice(head // 2 * 128, head // 2 * 128 + 128)
        kc, vc = k_ref[:, lanes], v_ref[:, lanes]
        qq = q_ref[:, lanes]
        if head % 2 == 0:
            kvs[head] = jnp.where(low, kc, swap_halves(vc))
        else:
            kvs[head] = jnp.where(low, swap_halves(kc), vc)
        for part in range(2):
            a = qq[part * tile : part * tile + half]
            b = qq[part * tile + half : (part + 1) * tile]
            if head % 2 == 0:
                packed = jnp.where(low_half, a, swap_halves(b))
            else:
                packed = jnp.where(low_half, swap_halves(a), b)
            qs[head, part] = packed
    kv_all[e] = kvs[z]
    q_all[e] = qs[z, x]
    lane = lax.broadcasted_iota(jnp.int32, (1, 128), 1)
    spread = jnp.where(
        lax.broadcasted_iota(jnp.int32, (16, 128), 0) + 64
        == lax.broadcasted_iota(jnp.int32, (16, 128), 1),
        1.0,
        0.0,
    )
    gate_lane = lax.broadcasted_iota(jnp.int32, (16, 128), 0) < 3
    spread = jnp.where(gate_lane, spread, 0.0).astype(jnp.bfloat16)
    pick_value = jnp.where(
        lax.broadcasted_iota(jnp.int32, (64, 128), 0) + 64
        == lax.broadcasted_iota(jnp.int32, (64, 128), 1),
        1.0,
        0.0,
    ).astype(jnp.bfloat16)
    unit = jnp.where(lane < 67, 1.0, 0.0).astype(jnp.bfloat16)
    both = (((1,), (1,)), ((), ()))

    def prep_kv(j):
        kv = kv_all[j]
        left = small_all[j, 8:16, :] * -LOG2E
        split = []
        for _ in range(3):
            piece = left.astype(jnp.bfloat16).astype(jnp.float32)
            split.append(jnp.concatenate([piece[r : r + 1] for r in range(lines)], axis=1))
            left = left - piece
        split.append(jnp.zeros((13, rows), jnp.float32))
        split = jnp.concatenate(split, axis=0).astype(jnp.bfloat16)
        gates = lax.dot_general(
            split, spread, (((0,), (0,)), ((), ())), preferred_element_type=jnp.float32
        )
        kg[j] = jnp.where(low, kv, gates.astype(jnp.bfloat16))
        vt[j] = lax.dot_general(
            pick_value, kv, both, preferred_element_type=jnp.float32
        ).astype(jnp.bfloat16)

    def prep_q(i):
        raw = q_all[i].astype(jnp.float32) * (LOG2E * 64**-0.5)
        first = raw.astype(jnp.bfloat16)
        second = (raw - first.astype(jnp.float32)).astype(jnp.bfloat16)
        zero = jnp.zeros_like(first)
        for n, (value, rest) in enumerate(((first, zero), (second, zero + unit))):
            qx[i, :, n * 128 : (n + 1) * 128] = jnp.concatenate(
                [jnp.where(low_half, value, rest), jnp.where(low_half, swap_halves(value), rest)],
                axis=0,
            )

    def scores_of(j, query):
        keys = jnp.concatenate([kv_all[j], kg[j]], axis=1)
        return lax.dot_general(keys, query, both, preferred_element_type=jnp.float32)

    def update(j, scores, peak, out):
        new_peak = jnp.maximum(peak, jnp.max(scores, axis=0, keepdims=True))
        weights = jnp.exp2(scores - new_peak).astype(jnp.bfloat16)
        out = out * jnp.exp2(peak - new_peak) + jnp.dot(
            vt[j], weights, preferred_element_type=jnp.float32
        )
        return new_peak, out

    def diagonal(k):
        pk = pair(k)
        first, second = qx[2 * pk], qx[2 * pk + 1]
        query = jnp.concatenate([first, second], axis=0)
        scores = scores_of(2 * pk, query)
        later = scores_of(2 * pk + 1, second)
        key_pos = lax.broadcasted_iota(jnp.int32, (rows, 2 * tile), 0)
        row_pos = lax.broadcasted_iota(jnp.int32, (rows, 2 * tile), 1)
        allowed = (key_pos <= row_pos + x * tile) | (row_pos >= tile)
        scores = jnp.where(allowed, scores, -jnp.inf)
        peak = jnp.max(scores, axis=0, keepdims=True)
        weights = jnp.exp2(scores - peak).astype(jnp.bfloat16)
        out = jnp.dot(vt[2 * pk], weights, preferred_element_type=jnp.float32)
        key_pos = lax.broadcasted_iota(jnp.int32, (rows, tile), 0)
        row_pos = lax.broadcasted_iota(jnp.int32, (rows, tile), 1)
        later = jnp.where(key_pos <= row_pos + x * tile, later, -jnp.inf)
        last_peak, last_out = update(2 * pk + 1, later, peak[:, tile:], out[:, tile:])
        peak_buf[pk, :, :tile] = peak[:, :tile]
        peak_buf[pk, :, tile:] = last_peak
        acc_buf[pk, :, :tile] = out[:, :tile]
        acc_buf[pk, :, tile:] = last_out

    def cross(k, m):
        pk, pm = pair(k), pair(m)
        above = (pk - pm + 4) // 4
        hi = pm + above * (pk - pm)
        lo = pk - above * (pk - pm)
        query = jnp.concatenate([qx[2 * hi], qx[2 * hi + 1]], axis=0)
        scores = scores_of(2 * lo, query)
        later = scores_of(2 * lo + 1, query)
        peak, out = update(2 * lo, scores, peak_buf[hi], acc_buf[hi])
        peak, out = update(2 * lo + 1, later, peak, out)
        peak_buf[hi] = peak
        acc_buf[hi] = out

    gain_pair = jnp.where(z // 2 == 0, gain_ref[:, :128], gain_ref[:, 128:])
    gain_swap = swap_halves(gain_pair)
    gain = jnp.where((lane < 64) == (lax.rem(z, 2) == 0), gain_pair, gain_swap)

    def epilogue(k):
        weighted = acc_buf[pair(k)]
        square = jnp.sum(weighted * weighted, axis=0, keepdims=True) / 64
        normed = weighted * lax.rsqrt(square + NORM_EPSILON)
        for xx in range(2):
            at = xx * tile
            out = jnp.concatenate(
                [normed[:, at : at + half], normed[:, at + half : at + tile]], axis=0
            ).T
            o_send[2 * pair(k) + xx] = (out * gain).astype(o_send.dtype)
        for m in (2 * k, 2 * k + 1):
            if m == 0:
                o_recv[e] = o_send[e]
            else:
                start(c_o, m)

    upper = (
        lax.broadcasted_iota(jnp.int32, (tokens, tokens), 0)
        <= lax.broadcasted_iota(jnp.int32, (tokens, tokens), 1)
    )
    upper = jnp.where(upper, 1.0, 0.0).astype(jnp.bfloat16)

    def select(k):
        pk = pair(k)
        named, chosen = [], []
        for bb in range(2):
            table = small_all[2 * pk + bb]
            ids_of = table[0:4].astype(jnp.int32)
            share = table[4:8]
            for j in range(per_group):
                hit = ids_of == e * per_group + j
                named.append(jnp.sum(jnp.where(hit, 1.0, 0.0), axis=0, keepdims=True))
                chosen.append(jnp.sum(jnp.where(hit, share, 0.0), axis=0, keepdims=True))
        flags = jnp.concatenate(named, axis=0)
        rank = jnp.dot(flags.astype(jnp.bfloat16), upper, preferred_element_type=jnp.float32)
        slot = jnp.where(flags > 0.5, rank - 1.0, -1000.0)
        row_of = lax.broadcasted_iota(jnp.int32, (slot2, 2 * tokens), 0).astype(jnp.float32)
        for j in range(per_group):
            target = jnp.concatenate(
                [slot[j : j + 1], slot[per_group + j : per_group + j + 1] + float(cap)], axis=1
            )
            share = jnp.concatenate([chosen[j], chosen[per_group + j]], axis=1)
            match = row_of == target
            sel_buf[k, j * slot2 : (j + 1) * slot2, :] = jnp.where(match, 1.0, 0.0).astype(
                jnp.bfloat16
            )
            share_buf[j, k * slot2 : (k + 1) * slot2, :] = jnp.sum(
                jnp.where(match, share, 0.0), axis=1, keepdims=True
            )

    def pick(k):
        gd0(k).wait_recv()
        gd1(k).wait_recv()
        pair_at = pl.ds(pl.multiple_of(pair(k) * 2 * tokens, 2 * tokens), 2 * tokens)
        for part in range(4):
            cols = slice(part * quarter, (part + 1) * quarter)
            picked = jnp.dot(
                sel_buf[k], x_all[pair_at, cols], preferred_element_type=jnp.float32
            ).astype(jnp.bfloat16)
            for j in range(per_group):
                xg[j, k * slot2 : (k + 1) * slot2, cols] = picked[j * slot2 : (j + 1) * slot2]

    def e1(k):
        gz(k).wait_recv()
        start(gx, k)

    def e2(k):
        gx(k).wait_recv()
        start(gy, k)
        start(gd0, k)

    def e3(k):
        gy(k).wait_recv()
        start(gd1, k)

    def forward(k):
        kvz(k).wait_recv()
        start(kvx, k)

    def ready(k):
        kvx(k).wait_recv()
        for m in (2 * k, 2 * k + 1):
            if m:
                qc(m).wait_recv()
            prep_kv(peer(m))
            prep_q(peer(m))

    for load in loads[9:12]:
        load.wait()
    shared_hidden = gated(x_all[own_rows, :], sgate[...], sup[...]).astype(jnp.bfloat16)
    for part in range(4):
        cols = slice(part * quarter, (part + 1) * quarter)
        ysh[part % 2, part // 2] = jnp.dot(
            shared_hidden, sdown[:, cols], preferred_element_type=jnp.float32
        ).astype(jnp.bfloat16)
    def experts_of(chunk):
        span = 2 * slot2

        @pl.loop(0, per_group, unroll=2)
        def _(j):
            here = slice(chunk * span, (chunk + 1) * span)
            value = gated(xg[j, here, :], egate[j], eup[j])
            hidden = (value * share_buf[j, here, :]).astype(jnp.bfloat16)
            at = pl.ds(pl.multiple_of(j * slot2, 16), slot2)
            for part in range(4):
                cols = slice(part * quarter, (part + 1) * quarter)
                out = jnp.dot(
                    hidden, edown[j, :, cols], preferred_element_type=jnp.float32
                ).astype(jnp.bfloat16)
                for k in range(2):
                    y_buf[part % 2, part // 2, 2 * chunk + k, at, :] = out[
                        k * slot2 : (k + 1) * slot2
                    ]

    def wide(ref):
        return ref.astype(jnp.float32)

    def core_sum(k):
        c_r1(k).wait_recv()
        s_send[k] = (wide(y_buf[c, 1 - y, k]) + wide(r1[1 - y, k])).astype(jnp.bfloat16)
        c_r2(k).start()

    def shared_sum():
        c_r1s().wait_recv()
        ss_send[...] = (wide(ysh[c, 1 - y]) + wide(r1s[1 - y])).astype(jnp.bfloat16)
        c_r2s().start()

    def scatter(k):
        c_r2(k).wait_recv()
        total = wide(y_buf[c, y, k]) + wide(r1[y, k]) + wide(r2[k])
        term = lax.dot_general(
            sel_buf[k],
            total.astype(jnp.bfloat16),
            (((0,), (0,)), ((), ())),
            preferred_element_type=jnp.float32,
        )
        term_buf[k, 0] = term[:tokens]
        term_buf[k, 1] = term[tokens:]
        t_send[k] = term_buf[k, 1 - x].astype(jnp.bfloat16)
        c_r3(k).start()

    def combine(k):
        c_r3(k).wait_recv()
        total = term_buf[k, x] + wide(r3[k])
        if k == 2:
            c_r4(3).wait_recv()
            total = total + wide(r4[3])
        u_send[k] = total.astype(jnp.bfloat16)
        c_r4(k).start()

    for k in range(4):
        started.append((c_r2, (k,)))
        started.append((c_r3, (k,)))
        if k:
            started.append((c_r4, (k,)))
    started.append((c_r2s, ()))

    start(c_r1s)
    for m in range(1, 8):
        small(m).wait_recv()
    for k in range(4):
        select(k)
    shared_sum()
    e2(0)
    e1(2)
    start(gz, 3)
    e1(1)
    for k in (3, 2, 1):
        start(kvz, k)
        start(qc, 2 * k)
    e3(0)
    e2(2)
    pick(0)
    e1(3)
    start(kvx, 0)
    for m in (1, 7, 5, 3):
        start(qc, m)
    e2(3)
    e2(1)
    e3(2)
    pick(2)
    ready(0)
    diagonal(0)
    forward(3)
    e3(3)
    for load in loads[12:]:
        load.wait()
    pick(3)
    experts_of(1)
    e3(1)
    start(c_r1, 3)
    start(c_r1, 2)
    ready(3)
    diagonal(3)
    core_sum(3)
    core_sum(2)
    pick(1)
    forward(2)
    experts_of(0)
    start(c_r1, 1)
    start(c_r1, 0)
    forward(1)
    ready(2)
    scatter(3)
    core_sum(1)
    core_sum(0)
    diagonal(2)
    cross(3, 0)
    scatter(2)
    combine(3)
    cross(2, 0)
    cross(2, 3)
    scatter(1)
    combine(2)
    ready(1)
    diagonal(1)
    scatter(0)
    cross(1, 3)
    epilogue(3)
    combine(1)
    cross(1, 2)
    epilogue(2)
    cross(1, 0)
    epilogue(1)
    epilogue(0)
    c_r2s().wait_recv()
    c_r3(0).wait_recv()
    out = term_buf[0, x] + wide(r3[0]) + wide(ysh[c, y]) + wide(r1s[y]) + wide(r2s[...])
    for k in (2, 1):
        c_r4(k).wait_recv()
        out = out + wide(r4[k])
    expert_ref[...] = out.astype(expert_ref.dtype)

    for m in range(1, 8):
        c_o(m).wait_recv()
    mixed_ref[...] = o_recv[...]
    for copy_fn, args in started:
        copy_fn(*args).wait_send()


def finish_kernel(parcels_ref, sum_ref, mixed_ref, expert_ref):
    count, half, _ = parcels_ref.shape
    low_half = lax.broadcasted_iota(jnp.int32, (half, 128), 1) < 64
    for part in range(2):
        for head in range(0, count // 2, 2):
            lanes = slice(head // 2 * 128, head // 2 * 128 + 128)
            first, second = parcels_ref[head * 2 + part], parcels_ref[(head + 1) * 2 + part]
            at = part * 2 * half
            mixed_ref[at : at + half, lanes] = jnp.where(low_half, first, swap_halves(second))
            mixed_ref[at + half : at + 2 * half, lanes] = jnp.where(
                low_half, swap_halves(first), second
            )
    expert_ref[...] = sum_ref[...]


def fused(
    queries,
    keys,
    values,
    cum_gate,
    head_gain,
    moe_in,
    ffn_gain,
    routes,
    route_weight,
    expert_gate,
    expert_up,
    expert_down,
    shared_gate,
    shared_up,
    shared_down,
):
    rows, heads = cum_gate.shape
    width = queries.shape[1]
    tokens, model = moe_in.shape
    choose = routes.shape[1]
    per_group, hid, _ = expert_gate.shape
    experts = per_group * lax.axis_size("ep")
    cap = 3 * tokens * choose // (2 * experts)
    devices = lax.axis_size("ep")
    tile, half, quarter = rows // 2, rows // 4, model // 4
    slots = per_group * 2 * cap
    shared = shared_gate.shape[0]
    bf16, f32 = jnp.bfloat16, jnp.float32
    vmem = pl.BlockSpec(memory_space=VMEM)
    hbm = pl.BlockSpec(memory_space=pl.ANY)
    scratch = [
        VMEM((tokens, model), bf16),
        VMEM((1, model), f32),
        VMEM((choose, tokens), jnp.int32),
        VMEM((choose, tokens), f32),
        VMEM((heads, rows), f32),
        VMEM((rows, width), bf16),
        VMEM((rows, width), bf16),
        VMEM((rows, width), bf16),
        VMEM((1, width), f32),
        VMEM((heads, 16, 128), f32),
        VMEM((heads, rows, 128), bf16),
        VMEM((heads, 2, half, 128), bf16),
        VMEM((devices, rows, 128), bf16),
        VMEM((devices, half, 128), bf16),
        VMEM((devices, rows, 128), bf16),
        VMEM((devices, 64, rows), bf16),
        VMEM((devices, tile, 256), bf16),
        VMEM((devices, 16, 128), f32),
        VMEM((4, 1, 2 * tile), f32),
        VMEM((4, 64, 2 * tile), f32),
        VMEM((devices, half, 128), bf16),
        VMEM((devices, half, 128), bf16),
        VMEM((devices * tokens, model), bf16),
        VMEM((per_group, 8 * cap, model), bf16),
        VMEM((4, slots, 2 * tokens), bf16),
        VMEM((per_group, 8 * cap, 1), f32),
        VMEM((per_group, hid, model), bf16),
        VMEM((per_group, hid, model), bf16),
        VMEM((per_group, hid, model), bf16),
        VMEM((shared, model), bf16),
        VMEM((shared, model), bf16),
        VMEM((shared, model), bf16),
        VMEM((2, 2, 4, slots, quarter), bf16),
        VMEM((2, 2, tokens, quarter), bf16),
        VMEM((2, 4, slots, quarter), bf16),
        VMEM((2, tokens, quarter), bf16),
        VMEM((4, slots, quarter), bf16),
        VMEM((tokens, quarter), bf16),
        VMEM((4, slots, quarter), bf16),
        VMEM((tokens, quarter), bf16),
        VMEM((4, 2, tokens, quarter), f32),
        VMEM((4, tokens, quarter), bf16),
        VMEM((4, tokens, quarter), bf16),
        VMEM((4, tokens, quarter), bf16),
        VMEM((4, tokens, quarter), bf16),
        pltpu.SemaphoreType.DMA((15,)),
        pltpu.SemaphoreType.DMA((COPIES,)),
        pltpu.SemaphoreType.DMA((COPIES,)),
    ]
    parcels, total = pl.pallas_call(
        functools.partial(fused_kernel, cap),
        in_specs=[hbm] * 15,
        out_specs=(vmem, vmem),
        out_shape=(
            jax.ShapeDtypeStruct((devices, half, 128), bf16),
            jax.ShapeDtypeStruct((tokens, quarter), bf16),
        ),
        scratch_shapes=scratch,
        compiler_params=pltpu.CompilerParams(
            collective_id=0, has_side_effects=True, vmem_limit_bytes=62 << 20
        ),
        name="fused",
    )(
        moe_in,
        ffn_gain[None],
        routes.T,
        route_weight.T,
        cum_gate.T,
        keys,
        values,
        queries,
        head_gain[None],
        expert_gate,
        expert_up,
        expert_down,
        shared_gate,
        shared_up,
        shared_down,
    )
    return pl.pallas_call(
        finish_kernel,
        in_specs=[vmem, vmem],
        out_specs=(vmem, vmem),
        out_shape=(
            jax.ShapeDtypeStruct((rows, width), bf16),
            jax.ShapeDtypeStruct((tokens, quarter), bf16),
        ),
        name="finish",
    )(parcels, total)


def fits_fused(cum_gate, queries, moe_in, routes, expert_gate):
    rows, heads = cum_gate.shape
    tokens, choose = routes.shape
    per_group = expert_gate.shape[0]
    devices = lax.axis_size("ep")
    cap = 3 * tokens * choose // (2 * per_group * devices)
    return (
        devices == 8
        and lax.axis_size("tp") == 4
        and heads == 4
        and queries.shape[1] == 256
        and rows % 128 == 0
        and rows // 128 <= 8
        and (rows // 4) % 16 == 0
        and tokens == 128
        and choose == 4
        and per_group == 4
        and (2 * cap) % 16 == 0
    )


def on_device(
    queries,
    keys,
    values,
    cum_gate,
    head_gain,
    moe_in,
    ffn_gain,
    routes,
    route_weight,
    expert_gate,
    expert_up,
    expert_down,
    shared_gate,
    shared_up,
    shared_down,
):
    if fits_fused(cum_gate, queries, moe_in, routes, expert_gate):
        return fused(
            queries,
            keys,
            values,
            cum_gate,
            head_gain,
            moe_in,
            ffn_gain,
            routes,
            route_weight,
            expert_gate,
            expert_up,
            expert_down,
            shared_gate,
            shared_up,
            shared_down,
        )
    rows, heads = cum_gate.shape
    gathered = gather_tokens(moe_in)
    got, packed = trade_rows(queries, keys, values, heads)
    all_gates, all_routes, all_weights = trade_small(cum_gate, routes, route_weight)
    gathered, got = lax.optimization_barrier((gathered, got))
    term = expert_terms(
        gathered,
        ffn_gain,
        all_routes,
        all_weights,
        expert_gate,
        expert_up,
        expert_down,
        shared_gate,
        shared_up,
        shared_down,
    )
    term, got = lax.optimization_barrier((term, got))
    mixed = attend(got, packed, rows, all_gates, heads, head_gain)
    return (mixed, combine_terms(term))


def solution(mesh):
    in_specs = (
        P("ep", "tp"),
        P("ep", "tp"),
        P("ep", "tp"),
        P("ep", "tp"),
        P("tp"),
        P("ep", None),
        P(),
        P("ep", None),
        P("ep", None),
        P("ep", "tp", None),
        P("ep", "tp", None),
        P("ep", "tp", None),
        P("tp", None),
        P("tp", None),
        P("tp", None),
    )
    out_specs = (P("ep", "tp"), P("ep", "tp"))
    return jax.shard_map(
        on_device, mesh=mesh, in_specs=in_specs, out_specs=out_specs, check_vma=False
    )
```
